32 devices in a mesh: dp: 4 (over y, x), kv: 4 (over z), tp: 2 (over core).
Axes of the slice: x: 2, y: 2, z: 4, core: 2. Of those that a mesh axis runs over, the one named last changes fastest.
Arguments:
- tokens: bfloat16 [4096, 2048], P(('dp', 'kv'), 'tp'), parts along dimension 0, may hold values from -6 to 6
- query_weight: bfloat16 [2048, 1024], P(None, 'tp'), may hold values from -2 to 2
- key_weight: bfloat16 [2048, 1024], P(None, 'tp'), may hold values from -2 to 2
- value_weight: bfloat16 [2048, 1024], P(None, 'tp'), may hold values from -0.125 to 0.125
- out_weight: bfloat16 [1024, 2048], P(None, 'tp'), may hold values from -0.75 to 0.75
- chosen: int32 [128, 16], P(('dp', 'kv')), parts along dimension 0, may hold values from -1 to 31, as said below
Outputs:
- mixed: bfloat16 [4096, 2048], P(('dp', 'kv'), 'tp'), parts along dimension 0
The draws below stay inside these ranges and needn't reach their ends.
There are 4 independent parts, one for each index of `dp`. The reference program is written for one: setup_inputs(seed, part) draws one part's arguments, and reference() takes and returns one part's arrays. A program takes and returns all parts, laid end to end along the dimension named above; an argument that names none is the same for every part. Nothing has to cross between parts.
Inputs may be any that keep to these rules, and one draw needn't show every extreme that they name: Each row of chosen lists distinct key blocks no later than its own query block, followed or mixed with -1 for empty slots; the own block is always listed, and block 0 too. For the 8 query blocks of one index of kv (aligned runs of rows), the distinct listed key blocks that lie among the 8 blocks of any one other index number at most 3, and exactly 3 for the index just before.
All inputs are finite; a program needn't handle non-finite values.
Results may differ from the reference program's by a relative error of at most 0.0084.
Values may be sent and summed in bfloat16 or wider, within the bound.
A program may use at most 128 MiB of HBM per device.

```python
import jax
import jax.numpy as jnp
from jax import lax

D = 2048
HEADS = 16
HEAD_DIM = 64
BLOCK = 32
TOPK = 16
CAP = 3
HW = 1024
BLK_DEV = 8
LEN = 1024
NBLK = 32


def paired_weights(key):
    first_key, second_key = jax.random.split(jax.random.fold_in(key, 5), 2)
    fan_scale = D ** (-0.5)
    base_draw = jax.random.normal(first_key, (D, HW), jnp.float32)
    other_draw = jax.random.normal(second_key, (D, HW), jnp.float32)
    query_part = base_draw
    key_part = other_draw
    return (jnp.clip(query_part * fan_scale, -2.0, 2.0), jnp.clip(key_part * fan_scale, -2.0, 2.0))


def draw_query_weight(key, part):
    return paired_weights(key)[0].astype(jnp.bfloat16)


def draw_key_weight(key, part):
    return paired_weights(key)[1].astype(jnp.bfloat16)


def draw_chosen(key, part):
    devices = NBLK // BLK_DEV
    key_popular, key_pick, key_score = jax.random.split(jax.random.fold_in(key, 11), 3)
    block_ids = jnp.arange(NBLK, dtype=jnp.int32)
    owner = block_ids // BLK_DEV
    local_index = block_ids % BLK_DEV
    popular = (jax.random.randint(key_popular, (NBLK,), 0, 8) == 0).astype(jnp.int32)
    asker = jnp.arange(devices, dtype=jnp.int32)[:, None]
    pick_score = jax.random.randint(key_pick, (devices, NBLK), 0, 4096) + popular[None, :] * 8192
    forced = (owner[None, :] == asker - 1) & (local_index[None, :] == BLK_DEV - 1) | (block_ids[None, :] == 0)
    pick_score = jnp.where(forced, 16384, pick_score) * BLK_DEV + (BLK_DEV - 1 - local_index)[None, :]
    pick_grid = pick_score.reshape(devices, devices, BLK_DEV)
    rank_in = jnp.sum((pick_grid[..., None, :] > pick_grid[..., :, None]).astype(jnp.int32), axis=-1)
    holder_ids = jnp.arange(devices, dtype=jnp.int32)
    allowed = (rank_in < CAP) & (holder_ids[None, :, None] < asker[:, :, None])
    allowed = allowed.reshape(devices, NBLK)
    query_block = block_ids[:, None]
    key_block = block_ids[None, :]
    query_owner = query_block // BLK_DEV
    local_ok = (key_block // BLK_DEV == query_owner) & (key_block <= query_block)
    remote_ok = allowed[query_owner[:, 0]]
    valid = local_ok | remote_ok
    mandatory = (key_block == query_block) | remote_ok & (key_block // BLK_DEV == query_owner - 1)
    mandatory = mandatory | (key_block == 0) & valid
    noise = jax.random.randint(key_score, (NBLK, NBLK), 0, 4096) + popular[None, :] * 4096
    score_int = jnp.where(mandatory, 16384, noise)
    score_int = jnp.where(valid, score_int * NBLK + key_block, -1)
    top_values, top_index = lax.top_k(score_int, TOPK)
    return jnp.where(top_values >= 0, top_index, -1).astype(jnp.int32)


def levels(own_key, shape, cuts, low, top_value):
    loudness, own = 1.0, jax.random.fold_in(own_key, 6)
    for position, parts in cuts:
        steps = jnp.exp(jax.random.uniform(jax.random.fold_in(own, position), (parts,), jnp.float32, low / len(cuts), top_value / len(cuts)))
        loudness = loudness * jnp.repeat(steps, shape[position] // parts).reshape([-1 if axis == position else 1 for axis in range(len(shape))])
    return loudness


def centred(rng, shape, spread, reach, cuts=(), kind=jnp.bfloat16):
    result = spread * jax.random.normal(rng, shape, jnp.float32)
    if cuts:
        result = result * levels(rng, shape, cuts, -0.22, 0.18)
    return jnp.clip(result, -reach, reach).astype(kind)


def setup_inputs(seed: int = 0, part: int = 0) -> dict:
    arg_keys = jax.random.split(jax.random.key(seed), 7)
    part_keys = jax.random.split(jax.random.fold_in(arg_keys[6], part), 7)
    return {
        "tokens": centred(part_keys[0], (LEN, D), 1.0, 6.0, ((0, 4), (1, 2))),
        "query_weight": draw_query_weight(jax.random.fold_in(arg_keys[6], 71), part),
        "key_weight": draw_key_weight(jax.random.fold_in(arg_keys[6], 71), part),
        "value_weight": centred(arg_keys[3], (D, HW), D ** -0.5, 0.125, ((1, 2),)),
        "out_weight": centred(arg_keys[4], (HW, D), (HW // 16) ** -0.5, 0.75, ((1, 2),)),
        "chosen": draw_chosen(jax.random.fold_in(jax.random.fold_in(arg_keys[6], part), 71), part),
    }


rotary_base = 500000.0
masked_score = -1e30


def rotate(heads_in, positions):
    half_dim = heads_in.shape[-1] // 2
    inverse = 1.0 / (rotary_base ** (jnp.arange(half_dim, dtype=jnp.float32) / half_dim))
    angles = positions.astype(jnp.float32)[:, None] * inverse[None, :]
    cosine = jnp.cos(angles)[:, None, :]
    sine_part = jnp.sin(angles)[:, None, :]
    first_half = heads_in[..., :half_dim]
    second_half = heads_in[..., half_dim:]
    return jnp.concatenate([first_half * cosine - second_half * sine_part,
                            first_half * sine_part + second_half * cosine], axis=-1)


def reference(tokens, query_weight, key_weight, value_weight, out_weight, chosen):
    length = tokens.shape[0]
    positions = jnp.arange(length, dtype=jnp.int32)
    heads_shape = (length, HEADS, HEAD_DIM)
    query_proj = rotate(jnp.dot(tokens, query_weight, preferred_element_type=jnp.float32).reshape(heads_shape),
                        positions).astype(jnp.bfloat16)
    key_proj = rotate(jnp.dot(tokens, key_weight, preferred_element_type=jnp.float32).reshape(heads_shape),
                      positions).astype(jnp.bfloat16)
    value_proj = jnp.dot(tokens, value_weight, preferred_element_type=jnp.float32).astype(jnp.bfloat16).reshape(heads_shape)
    blocks = length // BLOCK
    key_blocks = key_proj.reshape(blocks, BLOCK, HEADS, HEAD_DIM)
    value_blocks = value_proj.reshape(blocks, BLOCK, HEADS, HEAD_DIM)
    query_blocks = query_proj.reshape(blocks, BLOCK, HEADS, HEAD_DIM)
    score_scale = HEAD_DIM ** -0.5

    def one_block(inputs):
        query_block, listed, block_index = inputs
        safe_index = jnp.maximum(listed, 0).astype(jnp.int32)
        keys_sel = key_blocks[safe_index].reshape(TOPK * BLOCK, HEADS, HEAD_DIM).astype(jnp.float32)
        values_sel = value_blocks[safe_index].reshape(TOPK * BLOCK, HEADS, HEAD_DIM).astype(jnp.float32)
        key_pos = (safe_index[:, None] * BLOCK + jnp.arange(BLOCK, dtype=jnp.int32)[None, :]).reshape(-1)
        key_valid = jnp.repeat(listed >= 0, BLOCK)
        query_pos = block_index * BLOCK + jnp.arange(BLOCK, dtype=jnp.int32)
        allowed = key_valid[None, :] & (key_pos[None, :] <= query_pos[:, None])
        scores = jnp.einsum("qhd,khd->hqk", query_block.astype(jnp.float32), keys_sel) * score_scale
        scores = jnp.where(allowed[None], scores, masked_score)
        peak_row = jnp.max(scores, axis=2, keepdims=True)
        weights = jnp.where(allowed[None], jnp.exp(scores - peak_row), 0.0)
        denominator = jnp.sum(weights, axis=2)
        weight_low = lax.optimization_barrier(weights.astype(jnp.bfloat16))
        summed = jnp.einsum("hqk,khd->qhd", weight_low.astype(jnp.float32), values_sel)
        return (summed / denominator.T[:, :, None]).astype(jnp.bfloat16)

    attended = lax.map(one_block, (query_blocks, chosen, jnp.arange(blocks, dtype=jnp.int32)))
    attended = attended.reshape(length, HEADS * HEAD_DIM)
    return jnp.dot(attended, out_weight, preferred_element_type=jnp.float32).astype(jnp.bfloat16)
```

```python
import functools

import jax
import jax.numpy as jnp
import numpy as np
from jax import lax
from jax.experimental import pallas as pl
from jax.experimental.pallas import tpu as pltpu
from jax.sharding import PartitionSpec as P

HEAD_DIM = 64
BLOCK = 32
CAP = 3
LANES = 128
ROTARY_BASE = 500000.0
MASKED = -1e30
MESH = pl.DeviceIdType.MESH
F32 = jnp.float32
BF16 = jnp.bfloat16


def rotary_tables(rows, devices):
    half = HEAD_DIM // 2
    inverse = (1.0 / ROTARY_BASE ** (np.arange(half, dtype=np.float64) / half))
    lanes = np.tile(inverse, LANES // half)[None, :]
    row_angle = np.arange(rows, dtype=np.float64)[:, None] * lanes
    base_angle = (np.arange(devices, dtype=np.float64) * rows)[:, None] * lanes
    pack = lambda a: np.concatenate([np.cos(a), np.sin(a)], axis=1).astype(np.float32)
    return pack(row_angle), pack(base_angle)


def listed_columns(chosen, holder, rows):
    blocks = rows // BLOCK
    ids = holder * blocks + lax.broadcasted_iota(jnp.int32, (blocks, rows), 1) // BLOCK
    hit = jnp.zeros((blocks, rows), F32)
    for slot in range(chosen.shape[1]):
        hit = jnp.where(chosen[:, slot : slot + 1] == ids, 1.0, hit)
    return hit


def selection(hit, earlier):
    blocks, rows = hit.shape
    need = jnp.broadcast_to(jnp.max(hit, axis=0, keepdims=True), hit.shape)
    rank = jnp.dot(need.astype(BF16), earlier, preferred_element_type=F32)
    shape = (CAP * BLOCK, rows)
    slot_row = lax.broadcasted_iota(jnp.int32, shape, 0)
    column = lax.broadcasted_iota(jnp.int32, shape, 1)
    wanted = (slot_row // BLOCK).astype(F32)
    place = jnp.where(need[:1] > 0.5, rank[:1], -1.0)
    same = (slot_row % BLOCK) == (column % BLOCK)
    return jnp.where(same & (place == wanted), 1.0, 0.0).astype(BF16)


def layer(
    devices,
    chosen_hbm, base_hbm, row_hbm, tok_hbm, wq_hbm, wk_hbm, wv_hbm, wo_hbm,
    out_ref,
    chosen_ref, base_ref, tab, tok_own, tok_peer, wq, wk, wv, wo, q_acc, k_acc, v_acc, k_own, v_own, q2,
    lists, picks, k_rows, v_rows, far, peak, total, summed, mixed, att_own, att_peer,
    load_sem, tok_sem, att_sem, list_send, list_recv, key_send, key_recv, root_send, root_recv, pass_send,
):
    me = lax.axis_index("kv")
    core = lax.axis_index("tp")
    rows, half = tok_own.shape
    head_width = k_own.shape[1]
    pairs = head_width // LANES
    picked = CAP * BLOCK
    other = 1 - core

    loads = [
        pltpu.make_async_copy(src, dst, load_sem.at[i])
        for i, (src, dst) in enumerate(
            ((chosen_hbm, chosen_ref), (tok_hbm, tok_own), (wk_hbm, wk), (base_hbm, base_ref), (row_hbm, tab), (wv_hbm, wv), (wq_hbm, wq), (wo_hbm, wo))
        )
    ]
    for load in loads:
        load.start()
    chosen_load, tok_load, wk_load, base_load, tab_load, wv_load, wq_load, wo_load = loads

    barrier = pltpu.get_barrier_semaphore()
    pl.semaphore_signal(barrier, inc=1, device_id={"tp": other}, device_id_type=MESH)

    def greet(d, _):
        pl.semaphore_signal(
            barrier, inc=1, device_id={"kv": lax.rem(me + d, devices)}, device_id_type=MESH
        )
        return 0

    lax.fori_loop(1, devices, greet, 0)

    own_half = pl.ds(pl.multiple_of(core * half, half), half)
    peer_half = pl.ds(pl.multiple_of(other * half, half), half)

    def list_copy(d, target):
        return pltpu.make_async_remote_copy(
            src_ref=chosen_ref, dst_ref=lists.at[d], send_sem=list_send.at[d],
            recv_sem=list_recv.at[d], device_id={"kv": target}, device_id_type=MESH,
        )

    def send_list(d, _):
        list_copy(d, me - d).start()
        return 0

    tok_copy = pltpu.make_async_remote_copy(
        src_ref=tok_own, dst_ref=tok_peer, send_sem=tok_sem.at[0], recv_sem=tok_sem.at[1],
        device_id={"tp": other}, device_id_type=MESH,
    )

    chosen_load.wait()
    tok_load.wait()
    pl.semaphore_wait(barrier, devices)
    lax.fori_loop(1, me + 1, send_list, 0)
    tok_copy.start()

    wk_load.wait()
    k_acc[...] = jnp.dot(tok_own[...], wk[own_half, :], preferred_element_type=F32)
    wv_load.wait()
    v_acc[...] = jnp.dot(tok_own[...], wv[own_half, :], preferred_element_type=F32)
    wq_load.wait()
    q_acc[...] = jnp.dot(tok_own[...], wq[own_half, :], preferred_element_type=F32)

    tab_load.wait()
    base_load.wait()
    lane = lax.broadcasted_iota(jnp.int32, (rows, LANES), 1)
    first = (lane % HEAD_DIM) < HEAD_DIM // 2
    base = base_ref[pl.ds(me, 1), :]
    row_cos, row_sin = tab[:, :LANES], tab[:, LANES:]
    base_cos, base_sin = base[:, :LANES], base[:, LANES:]
    cosine = row_cos * base_cos - row_sin * base_sin
    sine = row_sin * base_cos + row_cos * base_sin
    sine = jnp.where(first, -sine, sine)
    tab[:, :LANES] = cosine
    tab[:, LANES:] = sine

    def rotated(x):
        swapped = jnp.where(
            first,
            pltpu.roll(x, LANES - HEAD_DIM // 2, axis=1),
            pltpu.roll(x, HEAD_DIM // 2, axis=1),
        )
        return x * tab[:, :LANES] + swapped * tab[:, LANES:]

    row_i = lax.broadcasted_iota(jnp.int32, (rows, rows), 0)
    col_i = lax.broadcasted_iota(jnp.int32, (rows, rows), 1)
    earlier = jnp.where((row_i % BLOCK == 0) & (row_i // BLOCK < col_i // BLOCK), 1.0, 0.0).astype(BF16)

    def choose(d, _):
        list_copy(d, me).wait_recv()
        picks[d] = selection(listed_columns(lists[d], me, rows), earlier)
        return 0

    lax.fori_loop(1, devices - me, choose, 0)

    buffers = ((k_own, k_rows), (v_own, v_rows))

    def row_copy(kind, i, d, target, holder):
        buffer = buffers[kind][1]

        def part(span):
            return pltpu.make_async_remote_copy(
                src_ref=buffer.at[lax.rem(me + d, devices), i, span], dst_ref=buffer.at[d, i, span],
                send_sem=key_send.at[kind, i, d], recv_sem=key_recv.at[kind, i, d],
                device_id={"kv": target}, device_id_type=MESH,
            )

        return part(slice(BLOCK, picked)), part(slice(0, picked)), holder == 0

    def each(copies, act):
        short, whole, is_short = copies
        pl.when(is_short)(lambda: act(short))
        pl.when(jnp.logical_not(is_short))(lambda: act(whole))

    relayed = devices > 2
    direct = devices - 2 if relayed else devices - 1
    relay_here = (me == devices - 2) if relayed else False

    def root_copy(kind, i, d, passing=False):
        own, buffer = buffers[kind]
        block = slice(0, BLOCK)
        return pltpu.make_async_remote_copy(
            src_ref=buffer.at[me, i, block] if passing else own.at[block, i * LANES : (i + 1) * LANES],
            dst_ref=buffer.at[d, i, block],
            send_sem=pass_send.at[kind, i] if passing else root_send.at[kind, i, d],
            recv_sem=root_recv.at[kind, i],
            device_id={"kv": lax.rem(d, devices)}, device_id_type=MESH,
        )

    def send_root(kind, some):
        @pl.when(me == 0)
        def _():
            def one(step, _):
                for i in some:
                    root_copy(kind, i, direct - step).start()
                return 0

            lax.fori_loop(0, direct, one, 0)

    def send_rows(kind, some):
        own, buffer = buffers[kind]
        columns = slice(some[0] * LANES, (some[-1] + 1) * LANES)

        def one(d, _):
            got = jnp.dot(picks[d], own[:, columns], preferred_element_type=F32).astype(BF16)
            for n, i in enumerate(some):
                buffer[me + d, i] = got[:, n * LANES : (n + 1) * LANES]
            for i in some:
                each(row_copy(kind, i, d, me + d, me), lambda c: c.start())
            return 0

        lax.fori_loop(1, devices - me, one, 0)

    tok_copy.wait_recv()
    step_pairs = 2 if pairs % 2 == 0 else 1
    for start in range(0, pairs, step_pairs):
        some = list(range(start, start + step_pairs))
        columns = slice(start * LANES, (start + step_pairs) * LANES)
        k_full = k_acc[:, columns] + jnp.dot(tok_peer[...], wk[peer_half, columns], preferred_element_type=F32)
        for n, i in enumerate(some):
            k_own[:, i * LANES : (i + 1) * LANES] = rotated(k_full[:, n * LANES : (n + 1) * LANES]).astype(BF16)
        send_root(0, some)
        send_rows(0, some)
        v_own[:, columns] = (
            v_acc[:, columns] + jnp.dot(tok_peer[...], wv[peer_half, columns], preferred_element_type=F32)
        ).astype(BF16)
        send_root(1, some)
        send_rows(1, some)

    q_full = q_acc[...] + jnp.dot(tok_peer[...], wq[peer_half, :], preferred_element_type=F32)
    for i in range(pairs):
        tile = slice(i * LANES, (i + 1) * LANES)
        q = rotated(q_full[:, tile]).astype(BF16).astype(F32) * (HEAD_DIM**-0.5)
        q2[i, :rows, :] = jnp.where(lane < HEAD_DIM, q, 0.0).astype(BF16)
        q2[i, rows:, :] = jnp.where(lane < HEAD_DIM, 0.0, q).astype(BF16)

    chosen = chosen_ref[...]

    def spread(hit):
        keys = hit.shape[1]
        blocks = hit.shape[0]
        wide = jnp.broadcast_to(hit[:, None, :], (blocks, BLOCK, keys))
        return wide.reshape(blocks * BLOCK, keys)

    def scores_of(i, keys):
        return lax.dot_general(
            q2[i], keys, (((1,), (1,)), ((), ())), preferred_element_type=F32
        )

    listed = spread(listed_columns(chosen, me, rows))
    bias = jnp.where((listed > 0.5) & (col_i <= row_i), 0.0, MASKED)
    bias = jnp.concatenate([bias, bias], axis=0)
    for i in range(pairs):
        tile = slice(i * LANES, (i + 1) * LANES)
        scores = scores_of(i, k_own[:, tile]) + bias
        top = jnp.max(scores, axis=1, keepdims=True)
        weights = jnp.exp(scores - top)
        peak[i] = jnp.broadcast_to(top, peak.shape[1:])
        total[i] = sum(weights[:, j : j + LANES] for j in range(0, rows, LANES))
        summed[i] = jnp.dot(weights.astype(BF16), v_own[:, tile], preferred_element_type=F32)

    def gauge(d, _):
        hit = listed_columns(chosen, me - d, rows)
        pick = selection(hit, earlier)
        got = lax.dot_general(
            hit.astype(BF16), pick, (((1,), (1,)), ((), ())), preferred_element_type=F32
        )
        far[d] = jnp.where(spread(got) > 0.5, 0.0, MASKED)
        return 0

    lax.fori_loop(1, me + 1, gauge, 0)

    if relayed:

        @pl.when(relay_here)
        def _():
            for i in range(pairs):
                for kind in range(2):
                    root_copy(kind, i, me).wait_recv()
                    root_copy(kind, i, devices - 1, True).start()

    def arrived(kind, i, d):
        each(row_copy(kind, i, d, me, me - d), lambda c: c.wait_recv())

        @pl.when((d == me) & jnp.logical_not(relay_here))
        def _():
            root_copy(kind, i, d).wait_recv()

    own_start = core * head_width
    peer_start = other * head_width

    def att_copy(i):
        return pltpu.make_async_remote_copy(
            src_ref=att_own.at[i], dst_ref=att_peer.at[i], send_sem=att_sem.at[0, i],
            recv_sem=att_sem.at[1, i], device_id={"tp": other}, device_id_type=MESH,
        )

    def project(i):
        att_copy(i).wait_recv()
        both = jnp.concatenate([att_own[i], att_peer[i]], axis=1)
        weight = jnp.concatenate(
            [
                wo[pl.ds(pl.multiple_of(start + i * LANES, LANES), LANES), :]
                for start in (own_start, peer_start)
            ],
            axis=0,
        )
        return jnp.dot(both, weight, preferred_element_type=F32)

    wo_load.wait()
    for i in range(pairs):

        def attend(step, _):
            d = jnp.where(step == 1, me, step - 1)
            arrived(0, i, d)
            bias = far[d]
            bias = jnp.concatenate([bias, bias], axis=0)
            scores = scores_of(i, k_rows[d, i]) + bias
            old = peak[i]
            top = jnp.maximum(old, jnp.max(scores, axis=1, keepdims=True))
            factor = jnp.exp(old - top)
            weights = jnp.exp(scores - top[:, :picked])
            peak[i] = top
            total[i] = total[i] * factor
            total[i, :, :picked] += weights
            arrived(1, i, d)
            summed[i] = summed[i] * factor + jnp.dot(
                weights.astype(BF16), v_rows[d, i], preferred_element_type=F32
            )
            return 0

        lax.fori_loop(1, me + 1, attend, 0)
        ratio = summed[i] / jnp.sum(total[i], axis=1, keepdims=True)
        att_own[i] = jnp.where(lane < HEAD_DIM, ratio[:rows], ratio[rows:]).astype(BF16)
        att_copy(i).start()
        if i == 1:
            mixed[...] = project(0)
        elif i > 1:
            mixed[...] += project(i - 1)
    last = project(pairs - 1)
    if pairs > 1:
        last = mixed[...] + last
    out_ref[...] = last.astype(BF16)

    for i in range(pairs):
        att_copy(i).wait_send()
    tok_copy.wait_send()

    def drain_list(d, _):
        list_copy(d, me - d).wait_send()
        return 0

    lax.fori_loop(1, me + 1, drain_list, 0)

    def drain_rows(d, _):
        for i in range(pairs):
            each(row_copy(0, i, d, me + d, me), lambda c: c.wait_send())
            each(row_copy(1, i, d, me + d, me), lambda c: c.wait_send())
        return 0

    lax.fori_loop(1, devices - me, drain_rows, 0)

    @pl.when(me == 0)
    def _():
        def drain_root(d, _):
            for i in range(pairs):
                root_copy(0, i, d).wait_send()
                root_copy(1, i, d).wait_send()
            return 0

        lax.fori_loop(1, direct + 1, drain_root, 0)

    if relayed:

        @pl.when(relay_here)
        def _():
            for i in range(pairs):
                for kind in range(2):
                    root_copy(kind, i, devices - 1, True).wait_send()


def on_device(devices, tokens, query_weight, key_weight, value_weight, out_weight, chosen):
    rows, half = tokens.shape
    width, head_width = query_weight.shape
    pairs = head_width // LANES
    picked = CAP * BLOCK
    row_table, base_table = rotary_tables(rows, devices)
    vmem = pl.BlockSpec(memory_space=pltpu.VMEM)
    anywhere = pl.BlockSpec(memory_space=pl.ANY)
    dma = pltpu.SemaphoreType.DMA
    return pl.pallas_call(
        functools.partial(layer, devices),
        out_shape=pltpu.VMEM((rows, out_weight.shape[1]), BF16),
        in_specs=[anywhere] * 8,
        out_specs=vmem,
        scratch_shapes=[
            pltpu.VMEM(chosen.shape, jnp.int32),
            pltpu.VMEM(base_table.shape, F32),
            pltpu.VMEM((rows, 2 * LANES), F32),
            pltpu.VMEM((rows, half), BF16),
            pltpu.VMEM((rows, half), BF16),
            pltpu.VMEM((width, head_width), BF16),
            pltpu.VMEM((width, head_width), BF16),
            pltpu.VMEM((width, head_width), BF16),
            pltpu.VMEM(out_weight.shape, BF16),
            pltpu.VMEM((rows, head_width), F32),
            pltpu.VMEM((rows, head_width), F32),
            pltpu.VMEM((rows, head_width), F32),
            pltpu.VMEM((rows, head_width), BF16),
            pltpu.VMEM((rows, head_width), BF16),
            pltpu.VMEM((pairs, 2 * rows, LANES), BF16),
            pltpu.VMEM((devices,) + chosen.shape, jnp.int32),
            pltpu.VMEM((devices, picked, rows), BF16),
            pltpu.VMEM((devices, pairs, picked, LANES), BF16),
            pltpu.VMEM((devices, pairs, picked, LANES), BF16),
            pltpu.VMEM((devices, rows, picked), F32),
            pltpu.VMEM((pairs, 2 * rows, LANES), F32),
            pltpu.VMEM((pairs, 2 * rows, LANES), F32),
            pltpu.VMEM((pairs, 2 * rows, LANES), F32),
            pltpu.VMEM((rows, out_weight.shape[1]), F32),
            pltpu.VMEM((pairs, rows, LANES), BF16),
            pltpu.VMEM((pairs, rows, LANES), BF16),
            dma((8,)),
            dma((2,)),
            dma((2, pairs)),
            dma((devices,)),
            dma((devices,)),
            dma((2, pairs, devices)),
            dma((2, pairs, devices)),
            dma((2, pairs, devices)),
            dma((2, pairs)),
            dma((2, pairs)),
        ],
        compiler_params=pltpu.CompilerParams(
            collective_id=0, has_side_effects=True, vmem_limit_bytes=62 * 1024 * 1024
        ),
        name="layer",
    )(
        chosen, jnp.asarray(base_table), jnp.asarray(row_table), tokens,
        query_weight, key_weight, value_weight, out_weight,
    )


def solution(mesh):
    placed = (
        P(("dp", "kv"), "tp"),
        P(None, "tp"),
        P(None, "tp"),
        P(None, "tp"),
        P(None, "tp"),
        P(("dp", "kv"), None),
    )
    return jax.shard_map(
        functools.partial(on_device, mesh.shape["kv"]),
        mesh=mesh, in_specs=placed, out_specs=P(("dp", "kv"), "tp"), check_vma=False,
    )
```

```python
import functools

import jax
import jax.numpy as jnp
import numpy as np
from jax import lax
from jax.experimental import pallas as pl
from jax.experimental.pallas import tpu as pltpu
from jax.sharding import PartitionSpec as P

HEAD_DIM = 64
BLOCK = 32
CAP = 3
LANES = 128
ROTARY_BASE = 500000.0
MASKED = -1e30
MESH = pl.DeviceIdType.MESH
F32 = jnp.float32
BF16 = jnp.bfloat16


def rotary_tables(rows, devices):
    half = HEAD_DIM // 2
    inverse = (1.0 / ROTARY_BASE ** (np.arange(half, dtype=np.float64) / half))
    lanes = np.tile(inverse, LANES // half)[None, :]
    row_angle = np.arange(rows, dtype=np.float64)[:, None] * lanes
    base_angle = (np.arange(devices, dtype=np.float64) * rows)[:, None] * lanes
    pack = lambda a: np.concatenate([np.cos(a), np.sin(a)], axis=1).astype(np.float32)
    return pack(row_angle), pack(base_angle)


def listed_columns(chosen, holder, rows):
    blocks = rows // BLOCK
    ids = holder * blocks + lax.broadcasted_iota(jnp.int32, (blocks, rows), 1) // BLOCK
    hit = jnp.zeros((blocks, rows), F32)
    for slot in range(chosen.shape[1]):
        hit = jnp.where(chosen[:, slot : slot + 1] == ids, 1.0, hit)
    return hit


def selection(hit, earlier, slots=CAP * BLOCK):
    blocks, rows = hit.shape
    need = jnp.broadcast_to(jnp.max(hit, axis=0, keepdims=True), hit.shape)
    rank = jnp.dot(need.astype(BF16), earlier, preferred_element_type=F32)
    shape = (slots, rows)
    slot_row = lax.broadcasted_iota(jnp.int32, shape, 0)
    column = lax.broadcasted_iota(jnp.int32, shape, 1)
    wanted = (slot_row // BLOCK).astype(F32)
    place = jnp.where(need[:1] > 0.5, rank[:1], -1.0)
    same = (slot_row % BLOCK) == (column % BLOCK)
    return jnp.where(same & (place == wanted), 1.0, 0.0).astype(BF16)


def layer(
    devices,
    chosen_hbm, base_hbm, row_hbm, tok_hbm, wq_hbm, wk_hbm, wv_hbm, wo_hbm,
    out_ref,
    chosen_ref, base_ref, tab, tok_own, tok_peer, wq, wk, wv, wo, q_acc, k_acc, v_acc, k_own, v_own, q2,
    lists, picks, k_rows, v_rows, raw, widest, peak, total, summed, weigh, att_own, att_peer,
    load_sem, tok_sem, att_sem, list_send, list_recv, key_send, key_recv, root_send, root_recv,
):
    me = lax.axis_index("kv")
    core = lax.axis_index("tp")
    rows, half = tok_own.shape
    head_width = k_own.shape[1]
    pairs = head_width // LANES
    picked = CAP * BLOCK
    other = 1 - core

    loads = [
        pltpu.make_async_copy(src, dst, load_sem.at[i])
        for i, (src, dst) in enumerate(
            ((chosen_hbm, chosen_ref), (base_hbm, base_ref), (tok_hbm, tok_own), (wk_hbm, wk), (row_hbm, tab), (wv_hbm, wv), (wq_hbm, wq), (wo_hbm, wo))
        )
    ]
    for load in loads:
        load.start()
    chosen_load, base_load, tok_load, wk_load, tab_load, wv_load, wq_load, wo_load = loads

    barrier = pltpu.get_barrier_semaphore()
    pl.semaphore_signal(barrier, inc=1, device_id={"tp": other}, device_id_type=MESH)

    def greet(d, _):
        pl.semaphore_signal(
            barrier, inc=1, device_id={"kv": lax.rem(me + d, devices)}, device_id_type=MESH
        )
        return 0

    lax.fori_loop(1, devices, greet, 0)

    own_half = pl.ds(pl.multiple_of(core * half, half), half)
    peer_half = pl.ds(pl.multiple_of(other * half, half), half)

    tok_load.wait()
    wk_load.wait()
    k_acc[...] = jnp.dot(tok_own[...], wk[own_half, :], preferred_element_type=F32)

    pl.semaphore_wait(barrier, devices)

    def list_copy(d, target):
        return pltpu.make_async_remote_copy(
            src_ref=chosen_ref, dst_ref=lists.at[d], send_sem=list_send.at[d],
            recv_sem=list_recv.at[d], device_id={"kv": target}, device_id_type=MESH,
        )

    def send_list(d, _):
        list_copy(d, me - d).start()
        return 0

    chosen_load.wait()
    lax.fori_loop(1, me + 1, send_list, 0)
    tok_copy = pltpu.make_async_remote_copy(
        src_ref=tok_own, dst_ref=tok_peer, send_sem=tok_sem.at[0], recv_sem=tok_sem.at[1],
        device_id={"tp": other}, device_id_type=MESH,
    )
    tok_copy.start()

    wv_load.wait()
    v_acc[...] = jnp.dot(tok_own[...], wv[own_half, :], preferred_element_type=F32)
    wq_load.wait()
    q_acc[...] = jnp.dot(tok_own[...], wq[own_half, :], preferred_element_type=F32)

    tab_load.wait()
    base_load.wait()
    lane = lax.broadcasted_iota(jnp.int32, (rows, LANES), 1)
    first = (lane % HEAD_DIM) < HEAD_DIM // 2
    base = base_ref[pl.ds(me, 1), :]
    row_cos, row_sin = tab[:, :LANES], tab[:, LANES:]
    base_cos, base_sin = base[:, :LANES], base[:, LANES:]
    cosine = row_cos * base_cos - row_sin * base_sin
    sine = row_sin * base_cos + row_cos * base_sin
    sine = jnp.where(first, -sine, sine)
    tab[:, :LANES] = cosine
    tab[:, LANES:] = sine

    def rotated(x):
        swapped = jnp.where(
            first,
            pltpu.roll(x, LANES - HEAD_DIM // 2, axis=1),
            pltpu.roll(x, HEAD_DIM // 2, axis=1),
        )
        return x * tab[:, :LANES] + swapped * tab[:, LANES:]

    row_i = lax.broadcasted_iota(jnp.int32, (rows, rows), 0)
    col_i = lax.broadcasted_iota(jnp.int32, (rows, rows), 1)
    earlier = jnp.where((row_i % BLOCK == 0) & (row_i // BLOCK < col_i // BLOCK), 1.0, 0.0).astype(BF16)

    tok_copy.wait_recv()
    k_full = k_acc[...] + jnp.dot(tok_peer[...], wk[peer_half, :], preferred_element_type=F32)
    for i in range(pairs):
        tile = slice(i * LANES, (i + 1) * LANES)
        k_own[:, tile] = rotated(k_full[:, tile]).astype(BF16)

    buffers = ((k_own, k_rows), (v_own, v_rows))

    def row_copy(kind, d, target, holder):
        buffer = buffers[kind][1]

        def part(span):
            return pltpu.make_async_remote_copy(
                src_ref=buffer.at[lax.rem(me + d, devices), span], dst_ref=buffer.at[d, span],
                send_sem=key_send.at[kind, d], recv_sem=key_recv.at[kind, d],
                device_id={"kv": target}, device_id_type=MESH,
            )

        return part(slice(BLOCK, picked)), part(slice(0, picked)), holder == 0

    def each(copies, act):
        short, whole, is_short = copies
        pl.when(is_short)(lambda: act(short))
        pl.when(jnp.logical_not(is_short))(lambda: act(whole))

    relayed = devices > 2
    direct = devices - 2 if relayed else devices - 1
    relay_here = (me == devices - 2) if relayed else False

    def root_copy(kind, d, passing=False):
        own, buffer = buffers[kind]
        block = slice(0, BLOCK)
        return pltpu.make_async_remote_copy(
            src_ref=buffer.at[me, block] if passing else own.at[block], dst_ref=buffer.at[d, block],
            send_sem=root_send.at[kind, d], recv_sem=root_recv.at[kind],
            device_id={"kv": lax.rem(d, devices)}, device_id_type=MESH,
        )

    def send_root(kind):
        @pl.when(me == 0)
        def _():
            def one(step, _):
                root_copy(kind, direct - step).start()
                return 0

            lax.fori_loop(0, direct, one, 0)

    def arrived(kind, d):
        each(row_copy(kind, d, me, me - d), lambda c: c.wait_recv())

        @pl.when((d == me) & jnp.logical_not(relay_here))
        def _():
            root_copy(kind, d).wait_recv()

    send_root(0)

    def send_keys(d, _):
        list_copy(d, me).wait_recv()
        pick = selection(listed_columns(lists[d], me, rows), earlier)
        picks[d] = pick
        k_rows[me + d] = jnp.dot(pick, k_own[...], preferred_element_type=F32).astype(BF16)
        each(row_copy(0, d, me + d, me), lambda c: c.start())
        return 0

    lax.fori_loop(1, devices - me, send_keys, 0)

    v_own[...] = (
        v_acc[...] + jnp.dot(tok_peer[...], wv[peer_half, :], preferred_element_type=F32)
    ).astype(BF16)

    send_root(1)

    def send_values(step, _):
        d = devices - 1 - me - step
        v_rows[me + d] = jnp.dot(picks[d], v_own[...], preferred_element_type=F32).astype(BF16)
        each(row_copy(1, d, me + d, me), lambda c: c.start())
        return 0

    lax.fori_loop(0, devices - 1 - me, send_values, 0)

    q_full = q_acc[...] + jnp.dot(tok_peer[...], wq[peer_half, :], preferred_element_type=F32)
    for i in range(pairs):
        tile = slice(i * LANES, (i + 1) * LANES)
        q = rotated(q_full[:, tile]).astype(BF16).astype(F32) * (HEAD_DIM**-0.5)
        q2[i, :rows, :] = jnp.where(lane < HEAD_DIM, q, 0.0).astype(BF16)
        q2[i, rows:, :] = jnp.where(lane < HEAD_DIM, 0.0, q).astype(BF16)

    chosen = chosen_ref[...]

    def spread(hit):
        keys = hit.shape[1]
        blocks = hit.shape[0]
        wide = jnp.broadcast_to(hit[:, None, :], (blocks, BLOCK, keys))
        return wide.reshape(blocks * BLOCK, keys)

    def scores_of(i, keys):
        return lax.dot_general(
            q2[i], keys, (((1,), (1,)), ((), ())), preferred_element_type=F32
        )

    def gauge(d, _):
        hit = listed_columns(chosen, me - d, rows)
        pick = selection(hit, earlier)
        got = lax.dot_general(
            hit.astype(BF16), pick, (((1,), (1,)), ((), ())), preferred_element_type=F32
        )
        far = jnp.where(spread(got) > 0.5, 0.0, MASKED)
        far = jnp.concatenate([far, far], axis=0)
        arrived(0, d)
        for i in range(pairs):
            tile = slice(i * LANES, (i + 1) * LANES)
            scores = scores_of(i, k_rows[d, :, tile]) + far
            raw[d - 1, i] = scores
            widest[i] = jnp.maximum(widest[i], scores)
        return 0

    listed = spread(listed_columns(chosen, me, rows))
    bias = jnp.where((listed > 0.5) & (col_i <= row_i), 0.0, MASKED)
    bias = jnp.concatenate([bias, bias], axis=0)
    for i in range(pairs):
        tile = slice(i * LANES, (i + 1) * LANES)
        scores = scores_of(i, k_own[:, tile]) + bias
        top = jnp.max(scores, axis=1, keepdims=True)
        weights = jnp.exp(scores - top)
        peak[i] = jnp.broadcast_to(top, peak.shape[1:])
        total[i] = sum(weights[:, j : j + LANES] for j in range(0, rows, LANES))
        summed[i] = jnp.dot(weights.astype(BF16), v_own[:, tile], preferred_element_type=F32)
        widest[i] = jnp.full(widest.shape[1:], MASKED, F32)

    if relayed:

        @pl.when(relay_here)
        def _():
            for kind in range(2):
                root_copy(kind, me).wait_recv()
                root_copy(kind, devices - 1, True).start()

    lax.fori_loop(1, me + 1, gauge, 0)

    @pl.when(me > 0)
    def _():
        for i in range(pairs):
            old = peak[i]
            top = jnp.maximum(old, jnp.max(widest[i], axis=1, keepdims=True))
            factor = jnp.exp(old - top)
            peak[i] = top
            total[i] = total[i] * factor
            summed[i] = summed[i] * factor

    def attend(step, _):
        d = jnp.where(me == devices - 1, step, me + 1 - step)
        for i in range(pairs):
            weights = jnp.exp(raw[d - 1, i] - peak[i, :, :picked])
            total[i, :, :picked] += weights
            weigh[i] = weights.astype(BF16)
        arrived(1, d)
        for i in range(pairs):
            tile = slice(i * LANES, (i + 1) * LANES)
            summed[i] += jnp.dot(weigh[i], v_rows[d, :, tile], preferred_element_type=F32)
        return 0

    lax.fori_loop(1, me + 1, attend, 0)

    att_copies = []
    for i in range(pairs):
        ratio = summed[i] / jnp.sum(total[i], axis=1, keepdims=True)
        att_own[i] = jnp.where(lane < HEAD_DIM, ratio[:rows], ratio[rows:]).astype(BF16)
        att_copies.append(
            pltpu.make_async_remote_copy(
                src_ref=att_own.at[i], dst_ref=att_peer.at[i], send_sem=att_sem.at[0, i],
                recv_sem=att_sem.at[1, i], device_id={"tp": other}, device_id_type=MESH,
            )
        )
        att_copies[-1].start()
    wo_load.wait()
    own_rows = pl.ds(pl.multiple_of(core * head_width, head_width), head_width)
    peer_rows = pl.ds(pl.multiple_of(other * head_width, head_width), head_width)
    joined = lambda ref: jnp.concatenate([ref[i] for i in range(pairs)], axis=1)
    mixed = jnp.dot(joined(att_own), wo[own_rows, :], preferred_element_type=F32)
    for copy in att_copies:
        copy.wait_recv()
    mixed = mixed + jnp.dot(joined(att_peer), wo[peer_rows, :], preferred_element_type=F32)
    out_ref[...] = mixed.astype(BF16)

    for copy in att_copies:
        copy.wait_send()
    tok_copy.wait_send()

    def drain_list(d, _):
        list_copy(d, me - d).wait_send()
        return 0

    lax.fori_loop(1, me + 1, drain_list, 0)

    def drain_rows(d, _):
        each(row_copy(0, d, me + d, me), lambda c: c.wait_send())
        each(row_copy(1, d, me + d, me), lambda c: c.wait_send())
        return 0

    lax.fori_loop(1, devices - me, drain_rows, 0)

    @pl.when(me == 0)
    def _():
        def drain_root(d, _):
            root_copy(0, d).wait_send()
            root_copy(1, d).wait_send()
            return 0

        lax.fori_loop(1, direct + 1, drain_root, 0)

    if relayed:

        @pl.when(relay_here)
        def _():
            for kind in range(2):
                root_copy(kind, devices - 1, True).wait_send()


def short_layer(
    devices,
    chosen_hbm, tab_hbm, tok_hbm, wq_hbm, wk_hbm, wv_hbm, wo_hbm,
    out_ref,
    chosen_ref, tab, tok_own, tok_peer, wq, wk, wv, wo, q_acc, k_acc, v_acc, k_own, v_own, q2,
    lists, picks, k_rows, v_rows, far, peak, total, summed, mixed, att_own, att_peer,
    load_sem, tok_send, tok_recv, att_send, att_recv, list_send, list_recv, key_send, key_recv, root_recv,
):
    me = lax.axis_index("kv")
    core = lax.axis_index("tp")
    rows, half = tok_own.shape
    pairs = k_own.shape[0]
    picked = CAP * BLOCK
    other = 1 - core
    relayed = devices > 2
    direct = devices - 2 if relayed else devices - 1
    span = 2 if pairs % 2 == 0 else 1
    groups = [list(range(start, start + span)) for start in range(0, pairs, span)]
    buffers = ((k_own, k_rows), (v_own, v_rows))

    loads = [
        pltpu.make_async_copy(src, dst, load_sem.at[i])
        for i, (src, dst) in enumerate(
            ((chosen_hbm, chosen_ref), (tok_hbm, tok_own), (wk_hbm, wk), (tab_hbm, tab), (wv_hbm, wv), (wq_hbm, wq), (wo_hbm, wo))
        )
    ]
    for load in loads:
        load.start()
    chosen_load, tok_load, wk_load, tab_load, wv_load, wq_load, wo_load = loads

    barrier = pltpu.get_barrier_semaphore()
    pl.semaphore_signal(barrier, inc=1, device_id={"tp": other}, device_id_type=MESH)
    for d in range(1, devices):
        pl.semaphore_signal(
            barrier, inc=1, device_id={"kv": lax.rem(me + d, devices)}, device_id_type=MESH
        )

    for _, buffer in buffers:
        for slot in range(devices - 1):
            empty = slice(slot * LANES + picked, (slot + 1) * LANES)
            buffer[:, empty, :] = jnp.zeros((pairs, LANES - picked, LANES), BF16)

    own_half = pl.ds(pl.multiple_of(core * half, half), half)
    peer_half = pl.ds(pl.multiple_of(other * half, half), half)

    def list_copy(d):
        return pltpu.make_async_remote_copy(
            src_ref=chosen_ref, dst_ref=lists.at[d - 1], send_sem=list_send.at[0],
            recv_sem=list_recv.at[d - 1], device_id={"kv": jnp.maximum(me - d, 0)}, device_id_type=MESH,
        )

    chunks = tok_recv.shape[0]
    chunk = rows // chunks

    def tok_copy(c):
        part = slice(c * chunk, (c + 1) * chunk)
        return pltpu.make_async_remote_copy(
            src_ref=tok_own.at[part], dst_ref=tok_peer.at[part], send_sem=tok_send.at[0],
            recv_sem=tok_recv.at[c], device_id={"tp": other}, device_id_type=MESH,
        )

    chosen_load.wait()
    tok_load.wait()
    pl.semaphore_wait(barrier, devices)
    for d in range(1, devices):
        pl.when(me >= d)(lambda d=d: list_copy(d).start())
    for c in range(chunks):
        tok_copy(c).start()

    wk_load.wait()
    k_acc[...] = jnp.dot(tok_own[...], wk[own_half, :], preferred_element_type=F32)
    wv_load.wait()
    v_acc[...] = jnp.dot(tok_own[...], wv[own_half, :], preferred_element_type=F32)
    wq_load.wait()
    q_acc[...] = jnp.dot(tok_own[...], wq[own_half, :], preferred_element_type=F32)

    tab_load.wait()
    lane = lax.broadcasted_iota(jnp.int32, (rows, LANES), 1)
    base = tab[pl.ds(rows + me, 1), :]
    row_cos, row_sin = tab[:rows, :LANES], tab[:rows, LANES:]
    base_cos, base_sin = base[:, :LANES], base[:, LANES:]
    cosine = row_cos * base_cos - row_sin * base_sin
    sine = row_sin * base_cos + row_cos * base_sin
    sine = jnp.where((lane % HEAD_DIM) < HEAD_DIM // 2, -sine, sine)
    tab[:rows, :LANES] = cosine
    tab[:rows, LANES:] = sine

    def rotated(x, part):
        first = (lax.broadcasted_iota(jnp.int32, x.shape, 1) % HEAD_DIM) < HEAD_DIM // 2
        swapped = jnp.where(
            first,
            pltpu.roll(x, LANES - HEAD_DIM // 2, axis=1),
            pltpu.roll(x, HEAD_DIM // 2, axis=1),
        )
        return x * tab[part, :LANES] + swapped * tab[part, LANES:]

    row_i = lax.broadcasted_iota(jnp.int32, (rows, rows), 0)
    col_i = lax.broadcasted_iota(jnp.int32, (rows, rows), 1)
    earlier = jnp.where((row_i % BLOCK == 0) & (row_i // BLOCK < col_i // BLOCK), 1.0, 0.0).astype(BF16)

    def choose(d, target):
        list_copy(d).wait_recv()
        slot = slice((target - 1) * LANES, target * LANES)
        picks[slot, :] = selection(listed_columns(lists[d - 1], me, rows), earlier, LANES)

    for m in range(devices - 1):

        @pl.when(me == m)
        def _(m=m):
            for d in range(1, devices - m):
                choose(d, m + d)

    def row_copy(kind, i, m, d):
        buffer = buffers[kind][1]
        low = BLOCK if m == 0 else 0
        return pltpu.make_async_remote_copy(
            src_ref=buffer.at[i, slice((m + d - 1) * LANES + low, (m + d - 1) * LANES + picked)],
            dst_ref=buffer.at[i, slice((d - 1) * LANES + low, (d - 1) * LANES + picked)],
            send_sem=key_send.at[kind], recv_sem=key_recv.at[kind, i],
            device_id={"kv": m + d}, device_id_type=MESH,
        )

    def root_copy(kind, g, d, passing=False):
        own, buffer = buffers[kind]
        some = slice(groups[g][0], groups[g][-1] + 1)
        here = lambda slot: buffer.at[some, slice((slot - 1) * LANES, (slot - 1) * LANES + BLOCK)]
        return pltpu.make_async_remote_copy(
            src_ref=here(devices - 2) if passing else own.at[some, slice(0, BLOCK)], dst_ref=here(d),
            send_sem=key_send.at[kind], recv_sem=root_recv.at[kind, g],
            device_id={"kv": d}, device_id_type=MESH,
        )

    def send(kind, g):
        own, buffer = buffers[kind]
        some = groups[g]

        @pl.when(me == 0)
        def _():
            for d in range(direct, 0, -1):
                root_copy(kind, g, d).start()

        for m in range(devices - 1):

            @pl.when(me == m)
            def _(m=m):
                wide = jnp.concatenate([own[i] for i in some], axis=1)
                got = jnp.dot(picks[m * LANES :, :], wide, preferred_element_type=F32).astype(BF16)
                for n, i in enumerate(some):
                    buffer[i, m * LANES :, :] = got[:, n * LANES : (n + 1) * LANES]
                for i in some:
                    for d in range(1, devices - m):
                        row_copy(kind, i, m, d).start()

    for g, some in enumerate(groups):
        columns = slice(some[0] * LANES, (some[-1] + 1) * LANES)
        parts = [slice(c * chunk, (c + 1) * chunk) for c in range(chunks)] if g == 0 else [slice(0, rows)]
        for c, part in enumerate(parts):
            if g == 0:
                tok_copy(c).wait_recv()
            k_full = k_acc[part, columns] + jnp.dot(
                tok_peer[part, :], wk[peer_half, columns], preferred_element_type=F32
            )
            for n, i in enumerate(some):
                k_own[i, part, :] = rotated(k_full[:, n * LANES : (n + 1) * LANES], part).astype(BF16)
        send(0, g)
        v_full = v_acc[:, columns] + jnp.dot(tok_peer[...], wv[peer_half, columns], preferred_element_type=F32)
        for n, i in enumerate(some):
            v_own[i] = v_full[:, n * LANES : (n + 1) * LANES].astype(BF16)
        send(1, g)

    q_full = q_acc[...] + jnp.dot(tok_peer[...], wq[peer_half, :], preferred_element_type=F32)
    for i in range(pairs):
        tile = slice(i * LANES, (i + 1) * LANES)
        q = rotated(q_full[:, tile], slice(0, rows)).astype(BF16).astype(F32) * (HEAD_DIM**-0.5)
        q2[i, :rows, :] = jnp.where(lane < HEAD_DIM, q, 0.0).astype(BF16)
        q2[i, rows:, :] = jnp.where(lane < HEAD_DIM, 0.0, q).astype(BF16)

    chosen = chosen_ref[...]

    def spread(hit):
        keys = hit.shape[1]
        blocks = hit.shape[0]
        wide = jnp.broadcast_to(hit[:, None, :], (blocks, BLOCK, keys))
        return wide.reshape(blocks * BLOCK, keys)

    def scores_of(i, keys):
        return lax.dot_general(
            q2[i], keys, (((1,), (1,)), ((), ())), preferred_element_type=F32
        )

    def lane_sums(weights):
        return sum(weights[:, j : j + LANES] for j in range(0, weights.shape[1], LANES))

    listed = spread(listed_columns(chosen, me, rows))
    bias = jnp.where((listed > 0.5) & (col_i <= row_i), 0.0, MASKED)
    bias = jnp.concatenate([bias, bias], axis=0)
    for i in range(pairs):
        scores = scores_of(i, k_own[i]) + bias
        top = jnp.max(scores, axis=1, keepdims=True)
        weights = jnp.exp(scores - top)
        peak[i] = jnp.broadcast_to(top, peak.shape[1:])
        total[i] = lane_sums(weights)
        summed[i] = jnp.dot(weights.astype(BF16), v_own[i], preferred_element_type=F32)

    for d in range(1, devices):

        @pl.when(me >= d)
        def _(d=d):
            hit = listed_columns(chosen, me - d, rows)
            pick = selection(hit, earlier, LANES)
            got = lax.dot_general(
                hit.astype(BF16), pick, (((1,), (1,)), ((), ())), preferred_element_type=F32
            )
            far[:, (d - 1) * LANES : d * LANES] = jnp.where(spread(got) > 0.5, 0.0, MASKED)

    def att_copy(i):
        return pltpu.make_async_remote_copy(
            src_ref=att_own.at[i], dst_ref=att_peer.at[i], send_sem=att_send.at[0],
            recv_sem=att_recv.at[i], device_id={"tp": other}, device_id_type=MESH,
        )

    def finish(i, result):
        att_own[i] = jnp.where(lane < HEAD_DIM, result[:rows], result[rows:]).astype(BF16)
        att_copy(i).start()

    def project(i):
        att_copy(i).wait_recv()
        both = jnp.concatenate([att_own[i], att_peer[i]], axis=1)
        weight = jnp.concatenate(
            [
                wo[pl.ds(pl.multiple_of((device * pairs + i) * LANES, LANES), LANES), :]
                for device in (core, other)
            ],
            axis=0,
        )
        return jnp.dot(both, weight, preferred_element_type=F32)

    def arrived(kind, i, m):
        buffer = buffers[kind][1]
        space = buffer.at[i, slice(0, m * picked - BLOCK)]
        pltpu.make_async_copy(space, space, key_recv.at[kind, i]).wait()

    def pass_root(g):
        for kind in range(2):
            root_copy(kind, g, devices - 2).wait_recv()
            root_copy(kind, g, devices - 1, True).start()

    wo_load.wait()
    for i in range(pairs):

        @pl.when(me == 0)
        def _(i=i):
            finish(i, summed[i] / jnp.sum(total[i], axis=1, keepdims=True))

        for m in range(1, devices):

            @pl.when(me == m)
            def _(i=i, m=m):
                opens = [g for g, some in enumerate(groups) if some[0] == i]
                passes = relayed and m == devices - 2
                if passes:
                    for g in range(len(groups)):
                        if g == i:
                            pass_root(g)
                else:
                    for g in opens:
                        root_copy(0, g, m).wait_recv()
                arrived(0, i, m)
                keys = slice(0, m * LANES)
                scores = scores_of(i, k_rows[i, keys, :]) + jnp.concatenate([far[:, keys], far[:, keys]], axis=0)
                old = peak[i]
                top = jnp.maximum(old, jnp.max(scores, axis=1, keepdims=True))
                factor = jnp.exp(old - top)
                weights = jnp.exp(scores - jnp.concatenate([top] * m, axis=1))
                inverse = 1.0 / jnp.sum(total[i] * factor + lane_sums(weights), axis=1, keepdims=True)
                before = summed[i] * (factor * inverse)
                weights = weights.astype(BF16)
                if not passes:
                    for g in opens:
                        root_copy(1, g, m).wait_recv()
                arrived(1, i, m)
                after = jnp.dot(weights, v_rows[i, keys, :], preferred_element_type=F32)
                finish(i, before + after * inverse)

        if i == 1:
            mixed[...] = project(0)
        elif i > 1:
            mixed[...] += project(i - 1)
    last = project(pairs - 1)
    if pairs > 1:
        last = mixed[...] + last
    out_ref[...] = last.astype(BF16)

    pltpu.make_async_copy(att_own, att_own, att_send.at[0]).wait()
    pltpu.make_async_copy(tok_own, tok_own, tok_send.at[0]).wait()
    for m in range(devices):

        @pl.when(me == m)
        def _(m=m):
            if m > 0:
                space = lists.at[slice(0, m)]
                pltpu.make_async_copy(space, space, list_send.at[0]).wait()
            sent = (devices - 1 - m) * (picked if m else picked - BLOCK)
            if m == 0:
                sent += direct * BLOCK
            elif relayed and m == devices - 2:
                sent += BLOCK
            if sent:
                for kind in range(2):
                    space = buffers[kind][1].at[:, slice(0, sent)]
                    pltpu.make_async_copy(space, space, key_send.at[kind]).wait()


def short_call(devices, tokens, query_weight, key_weight, value_weight, out_weight, chosen):
    rows, half = tokens.shape
    width, head_width = query_weight.shape
    pairs = head_width // LANES
    table = np.concatenate(rotary_tables(rows, devices), axis=0)
    vmem = pl.BlockSpec(memory_space=pltpu.VMEM)
    anywhere = pl.BlockSpec(memory_space=pl.ANY)
    dma = pltpu.SemaphoreType.DMA
    groups = pairs // 2 if pairs % 2 == 0 else pairs
    others = devices - 1
    return pl.pallas_call(
        functools.partial(short_layer, devices),
        out_shape=pltpu.VMEM((rows, out_weight.shape[1]), BF16),
        in_specs=[anywhere] * 7,
        out_specs=vmem,
        scratch_shapes=[
            pltpu.VMEM(chosen.shape, jnp.int32),
            pltpu.VMEM(table.shape, F32),
            pltpu.VMEM((rows, half), BF16),
            pltpu.VMEM((rows, half), BF16),
            pltpu.VMEM((width, head_width), BF16),
            pltpu.VMEM((width, head_width), BF16),
            pltpu.VMEM((width, head_width), BF16),
            pltpu.VMEM(out_weight.shape, BF16),
            pltpu.VMEM((rows, head_width), F32),
            pltpu.VMEM((rows, head_width), F32),
            pltpu.VMEM((rows, head_width), F32),
            pltpu.VMEM((pairs, rows, LANES), BF16),
            pltpu.VMEM((pairs, rows, LANES), BF16),
            pltpu.VMEM((pairs, 2 * rows, LANES), BF16),
            pltpu.VMEM((others,) + chosen.shape, jnp.int32),
            pltpu.VMEM((others * LANES, rows), BF16),
            pltpu.VMEM((pairs, others * LANES, LANES), BF16),
            pltpu.VMEM((pairs, others * LANES, LANES), BF16),
            pltpu.VMEM((rows, others * LANES), F32),
            pltpu.VMEM((pairs, 2 * rows, LANES), F32),
            pltpu.VMEM((pairs, 2 * rows, LANES), F32),
            pltpu.VMEM((pairs, 2 * rows, LANES), F32),
            pltpu.VMEM((rows, out_weight.shape[1]), F32),
            pltpu.VMEM((pairs, rows, LANES), BF16),
            pltpu.VMEM((pairs, rows, LANES), BF16),
            dma((7,)),
            dma((1,)),
            dma((2,)),
            dma((1,)),
            dma((pairs,)),
            dma((1,)),
            dma((others,)),
            dma((2,)),
            dma((2, pairs)),
            dma((2, groups)),
        ],
        compiler_params=pltpu.CompilerParams(
            collective_id=0, has_side_effects=True, vmem_limit_bytes=62 * 1024 * 1024
        ),
        name="layer",
    )(chosen, jnp.asarray(table), tokens, query_weight, key_weight, value_weight, out_weight)


def on_device(devices, tokens, query_weight, key_weight, value_weight, out_weight, chosen):
    rows, half = tokens.shape
    width, head_width = query_weight.shape
    pairs = head_width // LANES
    picked = CAP * BLOCK
    if devices <= 4:
        return short_call(devices, tokens, query_weight, key_weight, value_weight, out_weight, chosen)
    row_table, base_table = rotary_tables(rows, devices)
    vmem = pl.BlockSpec(memory_space=pltpu.VMEM)
    anywhere = pl.BlockSpec(memory_space=pl.ANY)
    dma = pltpu.SemaphoreType.DMA
    return pl.pallas_call(
        functools.partial(layer, devices),
        out_shape=pltpu.VMEM((rows, out_weight.shape[1]), BF16),
        in_specs=[anywhere] * 8,
        out_specs=vmem,
        scratch_shapes=[
            pltpu.VMEM(chosen.shape, jnp.int32),
            pltpu.VMEM(base_table.shape, F32),
            pltpu.VMEM((rows, 2 * LANES), F32),
            pltpu.VMEM((rows, half), BF16),
            pltpu.VMEM((rows, half), BF16),
            pltpu.VMEM((width, head_width), BF16),
            pltpu.VMEM((width, head_width), BF16),
            pltpu.VMEM((width, head_width), BF16),
            pltpu.VMEM(out_weight.shape, BF16),
            pltpu.VMEM((rows, head_width), F32),
            pltpu.VMEM((rows, head_width), F32),
            pltpu.VMEM((rows, head_width), F32),
            pltpu.VMEM((rows, head_width), BF16),
            pltpu.VMEM((rows, head_width), BF16),
            pltpu.VMEM((pairs, 2 * rows, LANES), BF16),
            pltpu.VMEM((devices,) + chosen.shape, jnp.int32),
            pltpu.VMEM((devices, picked, rows), BF16),
            pltpu.VMEM((devices, picked, head_width), BF16),
            pltpu.VMEM((devices, picked, head_width), BF16),
            pltpu.VMEM((devices - 1, pairs, 2 * rows, picked), F32),
            pltpu.VMEM((pairs, 2 * rows, picked), F32),
            pltpu.VMEM((pairs, 2 * rows, LANES), F32),
            pltpu.VMEM((pairs, 2 * rows, LANES), F32),
            pltpu.VMEM((pairs, 2 * rows, LANES), F32),
            pltpu.VMEM((pairs, 2 * rows, picked), BF16),
            pltpu.VMEM((pairs, rows, LANES), BF16),
            pltpu.VMEM((pairs, rows, LANES), BF16),
            dma((8,)),
            dma((2,)),
            dma((2, pairs)),
            dma((devices,)),
            dma((devices,)),
            dma((2, devices)),
            dma((2, devices)),
            dma((2, devices)),
            dma((2,)),
        ],
        compiler_params=pltpu.CompilerParams(
            collective_id=0, has_side_effects=True, vmem_limit_bytes=62 * 1024 * 1024
        ),
        name="layer",
    )(
        chosen, jnp.asarray(base_table), jnp.asarray(row_table), tokens,
        query_weight, key_weight, value_weight, out_weight,
    )


def solution(mesh):
    placed = (
        P(("dp", "kv"), "tp"),
        P(None, "tp"),
        P(None, "tp"),
        P(None, "tp"),
        P(None, "tp"),
        P(("dp", "kv"), None),
    )
    return jax.shard_map(
        functools.partial(on_device, mesh.shape["kv"]),
        mesh=mesh, in_specs=placed, out_specs=P(("dp", "kv"), "tp"), check_vma=False,
    )
```

```python
import functools

import jax
import jax.numpy as jnp
import numpy as np
from jax import lax
from jax.experimental import pallas as pl
from jax.experimental.pallas import tpu as pltpu
from jax.sharding import PartitionSpec as P

HEAD_DIM = 64
BLOCK = 32
CAP = 3
LANES = 128
ROTARY_BASE = 500000.0
MASKED = -1e30
MESH = pl.DeviceIdType.MESH
F32 = jnp.float32
BF16 = jnp.bfloat16


def rotary_tables(rows, devices):
    half = HEAD_DIM // 2
    inverse = (1.0 / ROTARY_BASE ** (np.arange(half, dtype=np.float64) / half))
    lanes = np.tile(inverse, LANES // half)[None, :]
    row_angle = np.arange(rows, dtype=np.float64)[:, None] * lanes
    base_angle = (np.arange(devices, dtype=np.float64) * rows)[:, None] * lanes
    pack = lambda a: np.concatenate([np.cos(a), np.sin(a)], axis=1).astype(np.float32)
    return pack(row_angle), pack(base_angle)


def listed_columns(chosen, holder, rows):
    blocks = rows // BLOCK
    ids = holder * blocks + lax.broadcasted_iota(jnp.int32, (blocks, rows), 1) // BLOCK
    hit = jnp.zeros((blocks, rows), F32)
    for slot in range(chosen.shape[1]):
        hit = jnp.where(chosen[:, slot : slot + 1] == ids, 1.0, hit)
    return hit


def selection(hit, earlier, slots=CAP * BLOCK):
    blocks, rows = hit.shape
    need = jnp.broadcast_to(jnp.max(hit, axis=0, keepdims=True), hit.shape)
    rank = jnp.dot(need.astype(BF16), earlier, preferred_element_type=F32)
    shape = (slots, rows)
    slot_row = lax.broadcasted_iota(jnp.int32, shape, 0)
    column = lax.broadcasted_iota(jnp.int32, shape, 1)
    wanted = (slot_row // BLOCK).astype(F32)
    place = jnp.where(need[:1] > 0.5, rank[:1], -1.0)
    same = (slot_row % BLOCK) == (column % BLOCK)
    return jnp.where(same & (place == wanted), 1.0, 0.0).astype(BF16)


def layer(
    devices,
    chosen_hbm, base_hbm, row_hbm, tok_hbm, wq_hbm, wk_hbm, wv_hbm, wo_hbm,
    out_ref,
    chosen_ref, base_ref, tab, tok_own, tok_peer, wq, wk, wv, wo, q_acc, k_acc, v_acc, k_own, v_own, q2,
    lists, picks, k_rows, v_rows, raw, widest, peak, total, summed, weigh, att_own, att_peer,
    load_sem, tok_sem, att_sem, list_send, list_recv, key_send, key_recv, root_send, root_recv,
):
    me = lax.axis_index("kv")
    core = lax.axis_index("tp")
    rows, half = tok_own.shape
    head_width = k_own.shape[1]
    pairs = head_width // LANES
    picked = CAP * BLOCK
    other = 1 - core

    loads = [
        pltpu.make_async_copy(src, dst, load_sem.at[i])
        for i, (src, dst) in enumerate(
            ((chosen_hbm, chosen_ref), (base_hbm, base_ref), (tok_hbm, tok_own), (wk_hbm, wk), (row_hbm, tab), (wv_hbm, wv), (wq_hbm, wq), (wo_hbm, wo))
        )
    ]
    for load in loads:
        load.start()
    chosen_load, base_load, tok_load, wk_load, tab_load, wv_load, wq_load, wo_load = loads

    barrier = pltpu.get_barrier_semaphore()
    pl.semaphore_signal(barrier, inc=1, device_id={"tp": other}, device_id_type=MESH)

    def greet(d, _):
        pl.semaphore_signal(
            barrier, inc=1, device_id={"kv": lax.rem(me + d, devices)}, device_id_type=MESH
        )
        return 0

    lax.fori_loop(1, devices, greet, 0)

    own_half = pl.ds(pl.multiple_of(core * half, half), half)
    peer_half = pl.ds(pl.multiple_of(other * half, half), half)

    tok_load.wait()
    wk_load.wait()
    k_acc[...] = jnp.dot(tok_own[...], wk[own_half, :], preferred_element_type=F32)

    pl.semaphore_wait(barrier, devices)

    def list_copy(d, target):
        return pltpu.make_async_remote_copy(
            src_ref=chosen_ref, dst_ref=lists.at[d], send_sem=list_send.at[d],
            recv_sem=list_recv.at[d], device_id={"kv": target}, device_id_type=MESH,
        )

    def send_list(d, _):
        list_copy(d, me - d).start()
        return 0

    chosen_load.wait()
    lax.fori_loop(1, me + 1, send_list, 0)
    tok_copy = pltpu.make_async_remote_copy(
        src_ref=tok_own, dst_ref=tok_peer, send_sem=tok_sem.at[0], recv_sem=tok_sem.at[1],
        device_id={"tp": other}, device_id_type=MESH,
    )
    tok_copy.start()

    wv_load.wait()
    v_acc[...] = jnp.dot(tok_own[...], wv[own_half, :], preferred_element_type=F32)
    wq_load.wait()
    q_acc[...] = jnp.dot(tok_own[...], wq[own_half, :], preferred_element_type=F32)

    tab_load.wait()
    base_load.wait()
    lane = lax.broadcasted_iota(jnp.int32, (rows, LANES), 1)
    first = (lane % HEAD_DIM) < HEAD_DIM // 2
    base = base_ref[pl.ds(me, 1), :]
    row_cos, row_sin = tab[:, :LANES], tab[:, LANES:]
    base_cos, base_sin = base[:, :LANES], base[:, LANES:]
    cosine = row_cos * base_cos - row_sin * base_sin
    sine = row_sin * base_cos + row_cos * base_sin
    sine = jnp.where(first, -sine, sine)
    tab[:, :LANES] = cosine
    tab[:, LANES:] = sine

    def rotated(x):
        swapped = jnp.where(
            first,
            pltpu.roll(x, LANES - HEAD_DIM // 2, axis=1),
            pltpu.roll(x, HEAD_DIM // 2, axis=1),
        )
        return x * tab[:, :LANES] + swapped * tab[:, LANES:]

    row_i = lax.broadcasted_iota(jnp.int32, (rows, rows), 0)
    col_i = lax.broadcasted_iota(jnp.int32, (rows, rows), 1)
    earlier = jnp.where((row_i % BLOCK == 0) & (row_i // BLOCK < col_i // BLOCK), 1.0, 0.0).astype(BF16)

    tok_copy.wait_recv()
    k_full = k_acc[...] + jnp.dot(tok_peer[...], wk[peer_half, :], preferred_element_type=F32)
    for i in range(pairs):
        tile = slice(i * LANES, (i + 1) * LANES)
        k_own[:, tile] = rotated(k_full[:, tile]).astype(BF16)

    buffers = ((k_own, k_rows), (v_own, v_rows))

    def row_copy(kind, d, target, holder):
        buffer = buffers[kind][1]

        def part(span):
            return pltpu.make_async_remote_copy(
                src_ref=buffer.at[lax.rem(me + d, devices), span], dst_ref=buffer.at[d, span],
                send_sem=key_send.at[kind, d], recv_sem=key_recv.at[kind, d],
                device_id={"kv": target}, device_id_type=MESH,
            )

        return part(slice(BLOCK, picked)), part(slice(0, picked)), holder == 0

    def each(copies, act):
        short, whole, is_short = copies
        pl.when(is_short)(lambda: act(short))
        pl.when(jnp.logical_not(is_short))(lambda: act(whole))

    relayed = devices > 2
    direct = devices - 2 if relayed else devices - 1
    relay_here = (me == devices - 2) if relayed else False

    def root_copy(kind, d, passing=False):
        own, buffer = buffers[kind]
        block = slice(0, BLOCK)
        return pltpu.make_async_remote_copy(
            src_ref=buffer.at[me, block] if passing else own.at[block], dst_ref=buffer.at[d, block],
            send_sem=root_send.at[kind, d], recv_sem=root_recv.at[kind],
            device_id={"kv": lax.rem(d, devices)}, device_id_type=MESH,
        )

    def send_root(kind):
        @pl.when(me == 0)
        def _():
            def one(step, _):
                root_copy(kind, direct - step).start()
                return 0

            lax.fori_loop(0, direct, one, 0)

    def arrived(kind, d):
        each(row_copy(kind, d, me, me - d), lambda c: c.wait_recv())

        @pl.when((d == me) & jnp.logical_not(relay_here))
        def _():
            root_copy(kind, d).wait_recv()

    send_root(0)

    def send_keys(d, _):
        list_copy(d, me).wait_recv()
        pick = selection(listed_columns(lists[d], me, rows), earlier)
        picks[d] = pick
        k_rows[me + d] = jnp.dot(pick, k_own[...], preferred_element_type=F32).astype(BF16)
        each(row_copy(0, d, me + d, me), lambda c: c.start())
        return 0

    lax.fori_loop(1, devices - me, send_keys, 0)

    v_own[...] = (
        v_acc[...] + jnp.dot(tok_peer[...], wv[peer_half, :], preferred_element_type=F32)
    ).astype(BF16)

    send_root(1)

    def send_values(step, _):
        d = devices - 1 - me - step
        v_rows[me + d] = jnp.dot(picks[d], v_own[...], preferred_element_type=F32).astype(BF16)
        each(row_copy(1, d, me + d, me), lambda c: c.start())
        return 0

    lax.fori_loop(0, devices - 1 - me, send_values, 0)

    q_full = q_acc[...] + jnp.dot(tok_peer[...], wq[peer_half, :], preferred_element_type=F32)
    for i in range(pairs):
        tile = slice(i * LANES, (i + 1) * LANES)
        q = rotated(q_full[:, tile]).astype(BF16).astype(F32) * (HEAD_DIM**-0.5)
        q2[i, :rows, :] = jnp.where(lane < HEAD_DIM, q, 0.0).astype(BF16)
        q2[i, rows:, :] = jnp.where(lane < HEAD_DIM, 0.0, q).astype(BF16)

    chosen = chosen_ref[...]

    def spread(hit):
        keys = hit.shape[1]
        blocks = hit.shape[0]
        wide = jnp.broadcast_to(hit[:, None, :], (blocks, BLOCK, keys))
        return wide.reshape(blocks * BLOCK, keys)

    def scores_of(i, keys):
        return lax.dot_general(
            q2[i], keys, (((1,), (1,)), ((), ())), preferred_element_type=F32
        )

    def gauge(d, _):
        hit = listed_columns(chosen, me - d, rows)
        pick = selection(hit, earlier)
        got = lax.dot_general(
            hit.astype(BF16), pick, (((1,), (1,)), ((), ())), preferred_element_type=F32
        )
        far = jnp.where(spread(got) > 0.5, 0.0, MASKED)
        far = jnp.concatenate([far, far], axis=0)
        arrived(0, d)
        for i in range(pairs):
            tile = slice(i * LANES, (i + 1) * LANES)
            scores = scores_of(i, k_rows[d, :, tile]) + far
            raw[d - 1, i] = scores
            widest[i] = jnp.maximum(widest[i], scores)
        return 0

    listed = spread(listed_columns(chosen, me, rows))
    bias = jnp.where((listed > 0.5) & (col_i <= row_i), 0.0, MASKED)
    bias = jnp.concatenate([bias, bias], axis=0)
    for i in range(pairs):
        tile = slice(i * LANES, (i + 1) * LANES)
        scores = scores_of(i, k_own[:, tile]) + bias
        top = jnp.max(scores, axis=1, keepdims=True)
        weights = jnp.exp(scores - top)
        peak[i] = jnp.broadcast_to(top, peak.shape[1:])
        total[i] = sum(weights[:, j : j + LANES] for j in range(0, rows, LANES))
        summed[i] = jnp.dot(weights.astype(BF16), v_own[:, tile], preferred_element_type=F32)
        widest[i] = jnp.full(widest.shape[1:], MASKED, F32)

    if relayed:

        @pl.when(relay_here)
        def _():
            for kind in range(2):
                root_copy(kind, me).wait_recv()
                root_copy(kind, devices - 1, True).start()

    lax.fori_loop(1, me + 1, gauge, 0)

    @pl.when(me > 0)
    def _():
        for i in range(pairs):
            old = peak[i]
            top = jnp.maximum(old, jnp.max(widest[i], axis=1, keepdims=True))
            factor = jnp.exp(old - top)
            peak[i] = top
            total[i] = total[i] * factor
            summed[i] = summed[i] * factor

    def attend(step, _):
        d = jnp.where(me == devices - 1, step, me + 1 - step)
        for i in range(pairs):
            weights = jnp.exp(raw[d - 1, i] - peak[i, :, :picked])
            total[i, :, :picked] += weights
            weigh[i] = weights.astype(BF16)
        arrived(1, d)
        for i in range(pairs):
            tile = slice(i * LANES, (i + 1) * LANES)
            summed[i] += jnp.dot(weigh[i], v_rows[d, :, tile], preferred_element_type=F32)
        return 0

    lax.fori_loop(1, me + 1, attend, 0)

    att_copies = []
    for i in range(pairs):
        ratio = summed[i] / jnp.sum(total[i], axis=1, keepdims=True)
        att_own[i] = jnp.where(lane < HEAD_DIM, ratio[:rows], ratio[rows:]).astype(BF16)
        att_copies.append(
            pltpu.make_async_remote_copy(
                src_ref=att_own.at[i], dst_ref=att_peer.at[i], send_sem=att_sem.at[0, i],
                recv_sem=att_sem.at[1, i], device_id={"tp": other}, device_id_type=MESH,
            )
        )
        att_copies[-1].start()
    wo_load.wait()
    own_rows = pl.ds(pl.multiple_of(core * head_width, head_width), head_width)
    peer_rows = pl.ds(pl.multiple_of(other * head_width, head_width), head_width)
    joined = lambda ref: jnp.concatenate([ref[i] for i in range(pairs)], axis=1)
    mixed = jnp.dot(joined(att_own), wo[own_rows, :], preferred_element_type=F32)
    for copy in att_copies:
        copy.wait_recv()
    mixed = mixed + jnp.dot(joined(att_peer), wo[peer_rows, :], preferred_element_type=F32)
    out_ref[...] = mixed.astype(BF16)

    for copy in att_copies:
        copy.wait_send()
    tok_copy.wait_send()

    def drain_list(d, _):
        list_copy(d, me - d).wait_send()
        return 0

    lax.fori_loop(1, me + 1, drain_list, 0)

    def drain_rows(d, _):
        each(row_copy(0, d, me + d, me), lambda c: c.wait_send())
        each(row_copy(1, d, me + d, me), lambda c: c.wait_send())
        return 0

    lax.fori_loop(1, devices - me, drain_rows, 0)

    @pl.when(me == 0)
    def _():
        def drain_root(d, _):
            root_copy(0, d).wait_send()
            root_copy(1, d).wait_send()
            return 0

        lax.fori_loop(1, direct + 1, drain_root, 0)

    if relayed:

        @pl.when(relay_here)
        def _():
            for kind in range(2):
                root_copy(kind, devices - 1, True).wait_send()


def short_layer(
    devices,
    chosen_hbm, tab_hbm, tok_hbm, wq_hbm, wk_hbm, wv_hbm, wo_hbm,
    out_ref,
    chosen_ref, tab, tok_own, tok_peer, wq, wk, wv, wo, q_acc, k_acc, v_acc, k_own, v_own, q2,
    lists, picks, k_rows, v_rows, far, peak, total, summed, weigh, mixed, att_own, att_peer, seed,
    load_sem, tok_send, tok_recv, att_send, att_recv, list_send, list_recv, key_send, key_recv, root_recv, seed_send, seed_recv, seed_ready,
):
    me = lax.axis_index("kv")
    core = lax.axis_index("tp")
    rows, half = tok_own.shape
    pairs = k_own.shape[0]
    picked = CAP * BLOCK
    other = 1 - core
    span = 2 if pairs % 2 == 0 else 1
    groups = [list(range(start, start + span)) for start in range(0, pairs, span)]
    buffers = ((k_own, k_rows), (v_own, v_rows))

    loads = [
        pltpu.make_async_copy(src, dst, load_sem.at[i])
        for i, (src, dst) in enumerate(
            ((chosen_hbm, chosen_ref), (tok_hbm, tok_own), (wk_hbm, wk), (tab_hbm, tab), (wv_hbm, wv), (wq_hbm, wq), (wo_hbm, wo))
        )
    ]
    for load in loads:
        load.start()
    chosen_load, tok_load, wk_load, tab_load, wv_load, wq_load, wo_load = loads

    barrier = pltpu.get_barrier_semaphore()
    pl.semaphore_signal(barrier, inc=1, device_id={"tp": other}, device_id_type=MESH)

    def greet(d, _):
        pl.semaphore_signal(barrier, inc=1, device_id={"kv": d}, device_id_type=MESH)
        return 0

    lax.fori_loop(me + 1, devices, greet, 0)

    for _, buffer in buffers:
        for slot in range(devices - 1):
            empty = slice(slot * LANES + picked, (slot + 1) * LANES)
            buffer[:, empty, :] = jnp.zeros((pairs, LANES - picked, LANES), BF16)

    own_half = pl.ds(pl.multiple_of(core * half, half), half)
    peer_half = pl.ds(pl.multiple_of(other * half, half), half)

    def list_copy(d):
        return pltpu.make_async_remote_copy(
            src_ref=chosen_ref, dst_ref=lists.at[d - 1], send_sem=list_send.at[0],
            recv_sem=list_recv.at[d - 1], device_id={"kv": jnp.maximum(me - d, 0)}, device_id_type=MESH,
        )

    chunks = tok_recv.shape[0]
    chunk = rows // chunks

    def tok_copy(c):
        part = slice(c * chunk, (c + 1) * chunk)
        return pltpu.make_async_remote_copy(
            src_ref=tok_own.at[part], dst_ref=tok_peer.at[part], send_sem=tok_send.at[0],
            recv_sem=tok_recv.at[c], device_id={"tp": other}, device_id_type=MESH,
        )

    chosen_load.wait()
    pl.semaphore_wait(barrier, 1 + me)
    for d in range(1, devices):
        pl.when(me >= d)(lambda d=d: list_copy(d).start())
    if devices > 2:

        @pl.when(me == 2)
        def _():
            pl.semaphore_signal(seed_ready, inc=1, device_id={"kv": 0}, device_id_type=MESH)

    tok_load.wait()
    for c in range(chunks):
        tok_copy(c).start()

    def seed_copy(source, target):
        return pltpu.make_async_remote_copy(
            src_ref=seed.at[0] if source else tok_own.at[slice(0, BLOCK)], dst_ref=seed.at[0],
            send_sem=seed_send.at[0], recv_sem=seed_recv.at[0],
            device_id={"kv": target}, device_id_type=MESH,
        )

    def seed_share():
        return pltpu.make_async_remote_copy(
            src_ref=seed.at[0], dst_ref=seed.at[1], send_sem=seed_send.at[1], recv_sem=seed_recv.at[1],
            device_id={"tp": other}, device_id_type=MESH,
        )

    wk_load.wait()
    k_acc[...] = jnp.dot(tok_own[...], wk[own_half, :], preferred_element_type=F32)
    wv_load.wait()
    v_acc[...] = jnp.dot(tok_own[...], wv[own_half, :], preferred_element_type=F32)
    wq_load.wait()
    q_acc[...] = jnp.dot(tok_own[...], wq[own_half, :], preferred_element_type=F32)

    if devices > 2:

        @pl.when(me == 0)
        def _():
            pl.semaphore_wait(seed_ready, 1)
            seed_copy(0, 2).start()

    tab_load.wait()
    lane = lax.broadcasted_iota(jnp.int32, (rows, LANES), 1)
    base = tab[pl.ds(rows + BLOCK + me, 1), :]
    row_cos, row_sin = tab[:rows, :LANES], tab[:rows, LANES:]
    base_cos, base_sin = base[:, :LANES], base[:, LANES:]
    cosine = row_cos * base_cos - row_sin * base_sin
    sine = row_sin * base_cos + row_cos * base_sin
    sine = jnp.where((lane % HEAD_DIM) < HEAD_DIM // 2, -sine, sine)
    tab[:rows, :LANES] = cosine
    tab[:rows, LANES:] = sine

    def rotated(x, part):
        first = (lax.broadcasted_iota(jnp.int32, x.shape, 1) % HEAD_DIM) < HEAD_DIM // 2
        swapped = jnp.where(
            first,
            pltpu.roll(x, LANES - HEAD_DIM // 2, axis=1),
            pltpu.roll(x, HEAD_DIM // 2, axis=1),
        )
        return x * tab[part, :LANES] + swapped * tab[part, LANES:]

    row_i = lax.broadcasted_iota(jnp.int32, (rows, rows), 0)
    col_i = lax.broadcasted_iota(jnp.int32, (rows, rows), 1)
    earlier = jnp.where((row_i % BLOCK == 0) & (row_i // BLOCK < col_i // BLOCK), 1.0, 0.0).astype(BF16)

    def choose(d, target):
        list_copy(d).wait_recv()
        slot = slice((target - 1) * LANES, target * LANES)
        picks[slot, :] = selection(listed_columns(lists[d - 1], me, rows), earlier, LANES)

    def row_copy(kind, i, m, d):
        buffer = buffers[kind][1]
        low = BLOCK if m == 0 else 0
        return pltpu.make_async_remote_copy(
            src_ref=buffer.at[i, slice((m + d - 1) * LANES + low, (m + d - 1) * LANES + picked)],
            dst_ref=buffer.at[i, slice((d - 1) * LANES + low, (d - 1) * LANES + picked)],
            send_sem=key_send.at[kind], recv_sem=key_recv.at[kind, i],
            device_id={"kv": m + d}, device_id_type=MESH,
        )

    def root_copy(kind, g):
        own, buffer = buffers[kind]
        some = slice(groups[g][0], groups[g][-1] + 1)
        return pltpu.make_async_remote_copy(
            src_ref=own.at[some, slice(0, BLOCK)], dst_ref=buffer.at[some, slice(0, BLOCK)],
            send_sem=key_send.at[kind], recv_sem=root_recv.at[kind, g],
            device_id={"kv": 1}, device_id_type=MESH,
        )

    def send(kind, g):
        own, buffer = buffers[kind]
        some = groups[g]

        def gather(low, high):
            wide = jnp.concatenate([own[i] for i in some], axis=1)
            span = slice((low - 1) * LANES, high * LANES)
            got = jnp.dot(picks[span, :], wide, preferred_element_type=F32).astype(BF16)
            for n, i in enumerate(some):
                buffer[i, span, :] = got[:, n * LANES : (n + 1) * LANES]

        for m in range(devices - 1):

            @pl.when(me == m)
            def _(m=m):
                targets = list(range(m + 1, devices))
                if kind == 0 and g == 0:
                    for t in targets:
                        choose(t - m, t)
                        gather(t, t)
                        for i in some:
                            row_copy(kind, i, m, t - m).start()
                else:
                    gather(m + 1, devices - 1)
                    for i in some:
                        for t in targets[1:] + targets[:1] if m == 0 else targets:
                            row_copy(kind, i, m, t - m).start()
                if m == 0:
                    root_copy(kind, g).start()

    for g, some in enumerate(groups):
        columns = slice(some[0] * LANES, (some[-1] + 1) * LANES)
        parts = [slice(c * chunk, (c + 1) * chunk) for c in range(chunks)] if g == 0 else [slice(0, rows)]
        for c, part in enumerate(parts):
            if g == 0:
                tok_copy(c).wait_recv()
            k_full = k_acc[part, columns] + jnp.dot(
                tok_peer[part, :], wk[peer_half, columns], preferred_element_type=F32
            )
            for n, i in enumerate(some):
                k_own[i, part, :] = rotated(k_full[:, n * LANES : (n + 1) * LANES], part).astype(BF16)
        if g == min(1, len(groups) - 1) and devices > 3:

            @pl.when(me == 2)
            def _():
                seed_copy(2, 2).wait_recv()
                seed_copy(2, 3).start()
                seed_share().start()

        send(0, g)
        v_full = v_acc[:, columns] + jnp.dot(tok_peer[...], wv[peer_half, columns], preferred_element_type=F32)
        for n, i in enumerate(some):
            v_own[i] = v_full[:, n * LANES : (n + 1) * LANES].astype(BF16)
        send(1, g)

    q_full = q_acc[...] + jnp.dot(tok_peer[...], wq[peer_half, :], preferred_element_type=F32)
    for i in range(pairs):
        tile = slice(i * LANES, (i + 1) * LANES)
        q = rotated(q_full[:, tile], slice(0, rows)).astype(BF16).astype(F32) * (HEAD_DIM**-0.5)
        q2[i, :rows, :] = jnp.where(lane < HEAD_DIM, q, 0.0).astype(BF16)
        q2[i, rows:, :] = jnp.where(lane < HEAD_DIM, 0.0, q).astype(BF16)

    chosen = chosen_ref[...]

    def spread(hit):
        keys = hit.shape[1]
        blocks = hit.shape[0]
        wide = jnp.broadcast_to(hit[:, None, :], (blocks, BLOCK, keys))
        return wide.reshape(blocks * BLOCK, keys)

    def scores_of(i, keys):
        return lax.dot_general(
            q2[i], keys, (((1,), (1,)), ((), ())), preferred_element_type=F32
        )

    def lane_sums(weights):
        return sum(weights[:, j : j + LANES] for j in range(0, weights.shape[1], LANES))

    listed = spread(listed_columns(chosen, me, rows))
    bias = jnp.where((listed > 0.5) & (col_i <= row_i), 0.0, MASKED)
    bias = jnp.concatenate([bias, bias], axis=0)
    for i in range(pairs):
        scores = scores_of(i, k_own[i]) + bias
        top = jnp.max(scores, axis=1, keepdims=True)
        weights = jnp.exp(scores - top)
        peak[i] = jnp.broadcast_to(top, peak.shape[1:])
        total[i] = lane_sums(weights)
        summed[i] = jnp.dot(weights.astype(BF16), v_own[i], preferred_element_type=F32)

    if devices > 2:

        @pl.when(me == devices - 1)
        def _():
            seed_copy(2, devices - 1).wait_recv()
            seed_share().start()

    for d in range(1, devices):

        @pl.when(me >= d)
        def _(d=d):
            hit = listed_columns(chosen, me - d, rows)
            pick = selection(hit, earlier, LANES)
            got = lax.dot_general(
                hit.astype(BF16), pick, (((1,), (1,)), ((), ())), preferred_element_type=F32
            )
            far[:, (d - 1) * LANES : d * LANES] = jnp.where(spread(got) > 0.5, 0.0, MASKED)

    def att_copy(i):
        return pltpu.make_async_remote_copy(
            src_ref=att_own.at[i], dst_ref=att_peer.at[i], send_sem=att_send.at[0],
            recv_sem=att_recv.at[i], device_id={"tp": other}, device_id_type=MESH,
        )

    def finish(i, result):
        att_own[i] = jnp.where(lane < HEAD_DIM, result[:rows], result[rows:]).astype(BF16)
        att_copy(i).start()

    def project(i):
        att_copy(i).wait_recv()
        both = jnp.concatenate([att_own[i], att_peer[i]], axis=1)
        weight = jnp.concatenate(
            [
                wo[pl.ds(pl.multiple_of((device * pairs + i) * LANES, LANES), LANES), :]
                for device in (core, other)
            ],
            axis=0,
        )
        return jnp.dot(both, weight, preferred_element_type=F32)

    def arrived(kind, i, m):
        buffer = buffers[kind][1]
        space = buffer.at[i, slice(0, m * picked - BLOCK)]
        pltpu.make_async_copy(space, space, key_recv.at[kind, i]).wait()

    if devices > 2:

        @pl.when(me >= 2)
        def _():
            seed_share().wait_recv()
            table = tab[rows : rows + BLOCK, :]
            first = (lax.broadcasted_iota(jnp.int32, (BLOCK, LANES), 1) % HEAD_DIM) < HEAD_DIM // 2
            block_cos = table[:, :LANES]
            block_sin = jnp.where(first, -table[:, LANES:], table[:, LANES:])
            for kind, weight in enumerate((wk, wv)):
                grown = jnp.dot(seed[0], weight[own_half, :], preferred_element_type=F32)
                grown = grown + jnp.dot(seed[1], weight[peer_half, :], preferred_element_type=F32)
                at = pl.ds(pl.multiple_of((me - 1) * LANES, LANES), BLOCK)
                for i in range(pairs):
                    x = grown[:, i * LANES : (i + 1) * LANES]
                    if kind == 0:
                        swapped = jnp.where(
                            first,
                            pltpu.roll(x, LANES - HEAD_DIM // 2, axis=1),
                            pltpu.roll(x, HEAD_DIM // 2, axis=1),
                        )
                        x = x * block_cos + swapped * block_sin
                    buffers[kind][1][i, at, :] = x.astype(BF16)

    def key_part(m, i, n):
        arrived(0, i, m)
        keys = slice(0, m * LANES)
        scores = scores_of(i, k_rows[i, keys, :]) + jnp.concatenate([far[:, keys], far[:, keys]], axis=0)
        old = peak[i]
        top = jnp.maximum(old, jnp.max(scores, axis=1, keepdims=True))
        factor = jnp.exp(old - top)
        weights = jnp.exp(scores - jnp.concatenate([top] * m, axis=1))
        inverse = 1.0 / jnp.sum(total[i] * factor + lane_sums(weights), axis=1, keepdims=True)
        summed[i] = summed[i] * (factor * inverse)
        total[i] = jnp.broadcast_to(inverse, total.shape[1:])
        weigh[n, :, keys] = weights.astype(BF16)

    def value_part(m, i, n):
        arrived(1, i, m)
        keys = slice(0, m * LANES)
        after = jnp.dot(weigh[n, :, keys], v_rows[i, keys, :], preferred_element_type=F32)
        finish(i, summed[i] + after * total[i])

    wo_load.wait()
    for g, some in enumerate(groups):
        for m in range(1, devices):

            @pl.when(me == m)
            def _(m=m, g=g, some=some):
                if m == 1:
                    root_copy(0, g).wait_recv()
                for n, i in enumerate(some):
                    key_part(m, i, n)

        if g > 0:
            for i in groups[g - 1]:
                if i == 0:
                    mixed[...] = project(i)
                else:
                    mixed[...] += project(i)

        @pl.when(me == 0)
        def _(some=some):
            for i in some:
                finish(i, summed[i] / jnp.sum(total[i], axis=1, keepdims=True))

        for m in range(1, devices):

            @pl.when(me == m)
            def _(m=m, g=g, some=some):
                if m == 1:
                    root_copy(1, g).wait_recv()
                for n, i in enumerate(some):
                    value_part(m, i, n)

    for i in groups[-1][:-1]:
        if i == 0:
            mixed[...] = project(i)
        else:
            mixed[...] += project(i)
    last = project(pairs - 1)
    if pairs > 1:
        last = mixed[...] + last
    out_ref[...] = last.astype(BF16)

    pltpu.make_async_copy(att_own, att_own, att_send.at[0]).wait()
    pltpu.make_async_copy(tok_own, tok_own, tok_send.at[0]).wait()
    for m in range(devices):

        @pl.when(me == m)
        def _(m=m):
            if m > 0:
                space = lists.at[slice(0, m)]
                pltpu.make_async_copy(space, space, list_send.at[0]).wait()
            sent = (devices - 1 - m) * (picked if m else picked - BLOCK)
            if m == 0:
                sent += BLOCK
            if devices > 2 and (m == 0 or 2 <= m < devices - 1):
                pltpu.make_async_copy(seed.at[0], seed.at[0], seed_send.at[0]).wait()
            if m >= 2:
                pltpu.make_async_copy(seed.at[0], seed.at[0], seed_send.at[1]).wait()
            if sent:
                for kind in range(2):
                    space = buffers[kind][1].at[:, slice(0, sent)]
                    pltpu.make_async_copy(space, space, key_send.at[kind]).wait()


def short_call(devices, tokens, query_weight, key_weight, value_weight, out_weight, chosen):
    rows, half = tokens.shape
    width, head_width = query_weight.shape
    pairs = head_width // LANES
    row_table, base_table = rotary_tables(rows, devices)
    table = np.concatenate([row_table, row_table[:BLOCK], base_table], axis=0)
    vmem = pl.BlockSpec(memory_space=pltpu.VMEM)
    anywhere = pl.BlockSpec(memory_space=pl.ANY)
    dma = pltpu.SemaphoreType.DMA
    groups = pairs // 2 if pairs % 2 == 0 else pairs
    others = devices - 1
    return pl.pallas_call(
        functools.partial(short_layer, devices),
        out_shape=pltpu.VMEM((rows, out_weight.shape[1]), BF16),
        in_specs=[anywhere] * 7,
        out_specs=vmem,
        scratch_shapes=[
            pltpu.VMEM(chosen.shape, jnp.int32),
            pltpu.VMEM(table.shape, F32),
            pltpu.VMEM((rows, half), BF16),
            pltpu.VMEM((rows, half), BF16),
            pltpu.VMEM((width, head_width), BF16),
            pltpu.VMEM((width, head_width), BF16),
            pltpu.VMEM((width, head_width), BF16),
            pltpu.VMEM(out_weight.shape, BF16),
            pltpu.VMEM((rows, head_width), F32),
            pltpu.VMEM((rows, head_width), F32),
            pltpu.VMEM((rows, head_width), F32),
            pltpu.VMEM((pairs, rows, LANES), BF16),
            pltpu.VMEM((pairs, rows, LANES), BF16),
            pltpu.VMEM((pairs, 2 * rows, LANES), BF16),
            pltpu.VMEM((others,) + chosen.shape, jnp.int32),
            pltpu.VMEM((others * LANES, rows), BF16),
            pltpu.VMEM((pairs, others * LANES, LANES), BF16),
            pltpu.VMEM((pairs, others * LANES, LANES), BF16),
            pltpu.VMEM((rows, others * LANES), F32),
            pltpu.VMEM((pairs, 2 * rows, LANES), F32),
            pltpu.VMEM((pairs, 2 * rows, LANES), F32),
            pltpu.VMEM((pairs, 2 * rows, LANES), F32),
            pltpu.VMEM((pairs // groups, 2 * rows, others * LANES), BF16),
            pltpu.VMEM((rows, out_weight.shape[1]), F32),
            pltpu.VMEM((pairs, rows, LANES), BF16),
            pltpu.VMEM((pairs, rows, LANES), BF16),
            pltpu.VMEM((2, BLOCK, half), BF16),
            dma((7,)),
            dma((1,)),
            dma((1,)),
            dma((1,)),
            dma((pairs,)),
            dma((1,)),
            dma((others,)),
            dma((2,)),
            dma((2, pairs)),
            dma((2, groups)),
            dma((2,)),
            dma((2,)),
            pltpu.SemaphoreType.REGULAR,
        ],
        compiler_params=pltpu.CompilerParams(
            collective_id=0, has_side_effects=True, vmem_limit_bytes=62 * 1024 * 1024
        ),
        name="layer",
    )(chosen, jnp.asarray(table), tokens, query_weight, key_weight, value_weight, out_weight)


def on_device(devices, tokens, query_weight, key_weight, value_weight, out_weight, chosen):
    rows, half = tokens.shape
    width, head_width = query_weight.shape
    pairs = head_width // LANES
    picked = CAP * BLOCK
    if devices <= 4:
        return short_call(devices, tokens, query_weight, key_weight, value_weight, out_weight, chosen)
    row_table, base_table = rotary_tables(rows, devices)
    vmem = pl.BlockSpec(memory_space=pltpu.VMEM)
    anywhere = pl.BlockSpec(memory_space=pl.ANY)
    dma = pltpu.SemaphoreType.DMA
    return pl.pallas_call(
        functools.partial(layer, devices),
        out_shape=pltpu.VMEM((rows, out_weight.shape[1]), BF16),
        in_specs=[anywhere] * 8,
        out_specs=vmem,
        scratch_shapes=[
            pltpu.VMEM(chosen.shape, jnp.int32),
            pltpu.VMEM(base_table.shape, F32),
            pltpu.VMEM((rows, 2 * LANES), F32),
            pltpu.VMEM((rows, half), BF16),
            pltpu.VMEM((rows, half), BF16),
            pltpu.VMEM((width, head_width), BF16),
            pltpu.VMEM((width, head_width), BF16),
            pltpu.VMEM((width, head_width), BF16),
            pltpu.VMEM(out_weight.shape, BF16),
            pltpu.VMEM((rows, head_width), F32),
            pltpu.VMEM((rows, head_width), F32),
            pltpu.VMEM((rows, head_width), F32),
            pltpu.VMEM((rows, head_width), BF16),
            pltpu.VMEM((rows, head_width), BF16),
            pltpu.VMEM((pairs, 2 * rows, LANES), BF16),
            pltpu.VMEM((devices,) + chosen.shape, jnp.int32),
            pltpu.VMEM((devices, picked, rows), BF16),
            pltpu.VMEM((devices, picked, head_width), BF16),
            pltpu.VMEM((devices, picked, head_width), BF16),
            pltpu.VMEM((devices - 1, pairs, 2 * rows, picked), F32),
            pltpu.VMEM((pairs, 2 * rows, picked), F32),
            pltpu.VMEM((pairs, 2 * rows, LANES), F32),
            pltpu.VMEM((pairs, 2 * rows, LANES), F32),
            pltpu.VMEM((pairs, 2 * rows, LANES), F32),
            pltpu.VMEM((pairs, 2 * rows, picked), BF16),
            pltpu.VMEM((pairs, rows, LANES), BF16),
            pltpu.VMEM((pairs, rows, LANES), BF16),
            dma((8,)),
            dma((2,)),
            dma((2, pairs)),
            dma((devices,)),
            dma((devices,)),
            dma((2, devices)),
            dma((2, devices)),
            dma((2, devices)),
            dma((2,)),
        ],
        compiler_params=pltpu.CompilerParams(
            collective_id=0, has_side_effects=True, vmem_limit_bytes=62 * 1024 * 1024
        ),
        name="layer",
    )(
        chosen, jnp.asarray(base_table), jnp.asarray(row_table), tokens,
        query_weight, key_weight, value_weight, out_weight,
    )


def solution(mesh):
    placed = (
        P(("dp", "kv"), "tp"),
        P(None, "tp"),
        P(None, "tp"),
        P(None, "tp"),
        P(None, "tp"),
        P(("dp", "kv"), None),
    )
    return jax.shard_map(
        functools.partial(on_device, mesh.shape["kv"]),
        mesh=mesh, in_specs=placed, out_specs=P(("dp", "kv"), "tp"), check_vma=False,
    )
```

```python
import functools

import jax
import jax.numpy as jnp
import numpy as np
from jax import lax
from jax.experimental import pallas as pl
from jax.experimental.pallas import tpu as pltpu
from jax.sharding import PartitionSpec as P

HEAD_DIM = 64
BLOCK = 32
CAP = 3
LANES = 128
ROTARY_BASE = 500000.0
MASKED = -1e30
MESH = pl.DeviceIdType.MESH
F32 = jnp.float32
BF16 = jnp.bfloat16


def rotary_tables(rows, devices):
    half = HEAD_DIM // 2
    inverse = (1.0 / ROTARY_BASE ** (np.arange(half, dtype=np.float64) / half))
    lanes = np.tile(inverse, LANES // half)[None, :]
    row_angle = np.arange(rows, dtype=np.float64)[:, None] * lanes
    base_angle = (np.arange(devices, dtype=np.float64) * rows)[:, None] * lanes
    pack = lambda a: np.concatenate([np.cos(a), np.sin(a)], axis=1).astype(np.float32)
    return pack(row_angle), pack(base_angle)


def listed_columns(chosen, holder, rows):
    blocks = rows // BLOCK
    ids = holder * blocks + lax.broadcasted_iota(jnp.int32, (blocks, rows), 1) // BLOCK
    hit = jnp.zeros((blocks, rows), F32)
    for slot in range(chosen.shape[1]):
        hit = jnp.where(chosen[:, slot : slot + 1] == ids, 1.0, hit)
    return hit


def selection(hit, earlier, slots=CAP * BLOCK):
    blocks, rows = hit.shape
    need = jnp.broadcast_to(jnp.max(hit, axis=0, keepdims=True), hit.shape)
    rank = jnp.dot(need.astype(BF16), earlier, preferred_element_type=F32)
    shape = (slots, rows)
    slot_row = lax.broadcasted_iota(jnp.int32, shape, 0)
    column = lax.broadcasted_iota(jnp.int32, shape, 1)
    wanted = (slot_row // BLOCK).astype(F32)
    place = jnp.where(need[:1] > 0.5, rank[:1], -1.0)
    same = (slot_row % BLOCK) == (column % BLOCK)
    return jnp.where(same & (place == wanted), 1.0, 0.0).astype(BF16)


def layer(
    devices,
    chosen_hbm, base_hbm, row_hbm, tok_hbm, wq_hbm, wk_hbm, wv_hbm, wo_hbm,
    out_ref,
    chosen_ref, base_ref, tab, tok_own, tok_peer, wq, wk, wv, wo, q_acc, k_acc, v_acc, k_own, v_own, q2,
    lists, picks, k_rows, v_rows, raw, widest, peak, total, summed, weigh, att_own, att_peer,
    load_sem, tok_sem, att_sem, list_send, list_recv, key_send, key_recv, root_send, root_recv,
):
    me = lax.axis_index("kv")
    core = lax.axis_index("tp")
    rows, half = tok_own.shape
    head_width = k_own.shape[1]
    pairs = head_width // LANES
    picked = CAP * BLOCK
    other = 1 - core

    loads = [
        pltpu.make_async_copy(src, dst, load_sem.at[i])
        for i, (src, dst) in enumerate(
            ((chosen_hbm, chosen_ref), (base_hbm, base_ref), (tok_hbm, tok_own), (wk_hbm, wk), (row_hbm, tab), (wv_hbm, wv), (wq_hbm, wq), (wo_hbm, wo))
        )
    ]
    for load in loads:
        load.start()
    chosen_load, base_load, tok_load, wk_load, tab_load, wv_load, wq_load, wo_load = loads

    barrier = pltpu.get_barrier_semaphore()
    pl.semaphore_signal(barrier, inc=1, device_id={"tp": other}, device_id_type=MESH)

    def greet(d, _):
        pl.semaphore_signal(
            barrier, inc=1, device_id={"kv": lax.rem(me + d, devices)}, device_id_type=MESH
        )
        return 0

    lax.fori_loop(1, devices, greet, 0)

    own_half = pl.ds(pl.multiple_of(core * half, half), half)
    peer_half = pl.ds(pl.multiple_of(other * half, half), half)

    tok_load.wait()
    wk_load.wait()
    k_acc[...] = jnp.dot(tok_own[...], wk[own_half, :], preferred_element_type=F32)

    pl.semaphore_wait(barrier, devices)

    def list_copy(d, target):
        return pltpu.make_async_remote_copy(
            src_ref=chosen_ref, dst_ref=lists.at[d], send_sem=list_send.at[d],
            recv_sem=list_recv.at[d], device_id={"kv": target}, device_id_type=MESH,
        )

    def send_list(d, _):
        list_copy(d, me - d).start()
        return 0

    chosen_load.wait()
    lax.fori_loop(1, me + 1, send_list, 0)
    tok_copy = pltpu.make_async_remote_copy(
        src_ref=tok_own, dst_ref=tok_peer, send_sem=tok_sem.at[0], recv_sem=tok_sem.at[1],
        device_id={"tp": other}, device_id_type=MESH,
    )
    tok_copy.start()

    wv_load.wait()
    v_acc[...] = jnp.dot(tok_own[...], wv[own_half, :], preferred_element_type=F32)
    wq_load.wait()
    q_acc[...] = jnp.dot(tok_own[...], wq[own_half, :], preferred_element_type=F32)

    tab_load.wait()
    base_load.wait()
    lane = lax.broadcasted_iota(jnp.int32, (rows, LANES), 1)
    first = (lane % HEAD_DIM) < HEAD_DIM // 2
    base = base_ref[pl.ds(me, 1), :]
    row_cos, row_sin = tab[:, :LANES], tab[:, LANES:]
    base_cos, base_sin = base[:, :LANES], base[:, LANES:]
    cosine = row_cos * base_cos - row_sin * base_sin
    sine = row_sin * base_cos + row_cos * base_sin
    sine = jnp.where(first, -sine, sine)
    tab[:, :LANES] = cosine
    tab[:, LANES:] = sine

    def rotated(x):
        swapped = jnp.where(
            first,
            pltpu.roll(x, LANES - HEAD_DIM // 2, axis=1),
            pltpu.roll(x, HEAD_DIM // 2, axis=1),
        )
        return x * tab[:, :LANES] + swapped * tab[:, LANES:]

    row_i = lax.broadcasted_iota(jnp.int32, (rows, rows), 0)
    col_i = lax.broadcasted_iota(jnp.int32, (rows, rows), 1)
    earlier = jnp.where((row_i % BLOCK == 0) & (row_i // BLOCK < col_i // BLOCK), 1.0, 0.0).astype(BF16)

    tok_copy.wait_recv()
    k_full = k_acc[...] + jnp.dot(tok_peer[...], wk[peer_half, :], preferred_element_type=F32)
    for i in range(pairs):
        tile = slice(i * LANES, (i + 1) * LANES)
        k_own[:, tile] = rotated(k_full[:, tile]).astype(BF16)

    buffers = ((k_own, k_rows), (v_own, v_rows))

    def row_copy(kind, d, target, holder):
        buffer = buffers[kind][1]

        def part(span):
            return pltpu.make_async_remote_copy(
                src_ref=buffer.at[lax.rem(me + d, devices), span], dst_ref=buffer.at[d, span],
                send_sem=key_send.at[kind, d], recv_sem=key_recv.at[kind, d],
                device_id={"kv": target}, device_id_type=MESH,
            )

        return part(slice(BLOCK, picked)), part(slice(0, picked)), holder == 0

    def each(copies, act):
        short, whole, is_short = copies
        pl.when(is_short)(lambda: act(short))
        pl.when(jnp.logical_not(is_short))(lambda: act(whole))

    relayed = devices > 2
    direct = devices - 2 if relayed else devices - 1
    relay_here = (me == devices - 2) if relayed else False

    def root_copy(kind, d, passing=False):
        own, buffer = buffers[kind]
        block = slice(0, BLOCK)
        return pltpu.make_async_remote_copy(
            src_ref=buffer.at[me, block] if passing else own.at[block], dst_ref=buffer.at[d, block],
            send_sem=root_send.at[kind, d], recv_sem=root_recv.at[kind],
            device_id={"kv": lax.rem(d, devices)}, device_id_type=MESH,
        )

    def send_root(kind):
        @pl.when(me == 0)
        def _():
            def one(step, _):
                root_copy(kind, direct - step).start()
                return 0

            lax.fori_loop(0, direct, one, 0)

    def arrived(kind, d):
        each(row_copy(kind, d, me, me - d), lambda c: c.wait_recv())

        @pl.when((d == me) & jnp.logical_not(relay_here))
        def _():
            root_copy(kind, d).wait_recv()

    send_root(0)

    def send_keys(d, _):
        list_copy(d, me).wait_recv()
        pick = selection(listed_columns(lists[d], me, rows), earlier)
        picks[d] = pick
        k_rows[me + d] = jnp.dot(pick, k_own[...], preferred_element_type=F32).astype(BF16)
        each(row_copy(0, d, me + d, me), lambda c: c.start())
        return 0

    lax.fori_loop(1, devices - me, send_keys, 0)

    v_own[...] = (
        v_acc[...] + jnp.dot(tok_peer[...], wv[peer_half, :], preferred_element_type=F32)
    ).astype(BF16)

    send_root(1)

    def send_values(step, _):
        d = devices - 1 - me - step
        v_rows[me + d] = jnp.dot(picks[d], v_own[...], preferred_element_type=F32).astype(BF16)
        each(row_copy(1, d, me + d, me), lambda c: c.start())
        return 0

    lax.fori_loop(0, devices - 1 - me, send_values, 0)

    q_full = q_acc[...] + jnp.dot(tok_peer[...], wq[peer_half, :], preferred_element_type=F32)
    for i in range(pairs):
        tile = slice(i * LANES, (i + 1) * LANES)
        q = rotated(q_full[:, tile]).astype(BF16).astype(F32) * (HEAD_DIM**-0.5)
        q2[i, :rows, :] = jnp.where(lane < HEAD_DIM, q, 0.0).astype(BF16)
        q2[i, rows:, :] = jnp.where(lane < HEAD_DIM, 0.0, q).astype(BF16)

    chosen = chosen_ref[...]

    def spread(hit):
        keys = hit.shape[1]
        blocks = hit.shape[0]
        wide = jnp.broadcast_to(hit[:, None, :], (blocks, BLOCK, keys))
        return wide.reshape(blocks * BLOCK, keys)

    def scores_of(i, keys):
        return lax.dot_general(
            q2[i], keys, (((1,), (1,)), ((), ())), preferred_element_type=F32
        )

    def gauge(d, _):
        hit = listed_columns(chosen, me - d, rows)
        pick = selection(hit, earlier)
        got = lax.dot_general(
            hit.astype(BF16), pick, (((1,), (1,)), ((), ())), preferred_element_type=F32
        )
        far = jnp.where(spread(got) > 0.5, 0.0, MASKED)
        far = jnp.concatenate([far, far], axis=0)
        arrived(0, d)
        for i in range(pairs):
            tile = slice(i * LANES, (i + 1) * LANES)
            scores = scores_of(i, k_rows[d, :, tile]) + far
            raw[d - 1, i] = scores
            widest[i] = jnp.maximum(widest[i], scores)
        return 0

    listed = spread(listed_columns(chosen, me, rows))
    bias = jnp.where((listed > 0.5) & (col_i <= row_i), 0.0, MASKED)
    bias = jnp.concatenate([bias, bias], axis=0)
    for i in range(pairs):
        tile = slice(i * LANES, (i + 1) * LANES)
        scores = scores_of(i, k_own[:, tile]) + bias
        top = jnp.max(scores, axis=1, keepdims=True)
        weights = jnp.exp(scores - top)
        peak[i] = jnp.broadcast_to(top, peak.shape[1:])
        total[i] = sum(weights[:, j : j + LANES] for j in range(0, rows, LANES))
        summed[i] = jnp.dot(weights.astype(BF16), v_own[:, tile], preferred_element_type=F32)
        widest[i] = jnp.full(widest.shape[1:], MASKED, F32)

    if relayed:

        @pl.when(relay_here)
        def _():
            for kind in range(2):
                root_copy(kind, me).wait_recv()
                root_copy(kind, devices - 1, True).start()

    lax.fori_loop(1, me + 1, gauge, 0)

    @pl.when(me > 0)
    def _():
        for i in range(pairs):
            old = peak[i]
            top = jnp.maximum(old, jnp.max(widest[i], axis=1, keepdims=True))
            factor = jnp.exp(old - top)
            peak[i] = top
            total[i] = total[i] * factor
            summed[i] = summed[i] * factor

    def attend(step, _):
        d = jnp.where(me == devices - 1, step, me + 1 - step)
        for i in range(pairs):
            weights = jnp.exp(raw[d - 1, i] - peak[i, :, :picked])
            total[i, :, :picked] += weights
            weigh[i] = weights.astype(BF16)
        arrived(1, d)
        for i in range(pairs):
            tile = slice(i * LANES, (i + 1) * LANES)
            summed[i] += jnp.dot(weigh[i], v_rows[d, :, tile], preferred_element_type=F32)
        return 0

    lax.fori_loop(1, me + 1, attend, 0)

    att_copies = []
    for i in range(pairs):
        ratio = summed[i] / jnp.sum(total[i], axis=1, keepdims=True)
        att_own[i] = jnp.where(lane < HEAD_DIM, ratio[:rows], ratio[rows:]).astype(BF16)
        att_copies.append(
            pltpu.make_async_remote_copy(
                src_ref=att_own.at[i], dst_ref=att_peer.at[i], send_sem=att_sem.at[0, i],
                recv_sem=att_sem.at[1, i], device_id={"tp": other}, device_id_type=MESH,
            )
        )
        att_copies[-1].start()
    wo_load.wait()
    own_rows = pl.ds(pl.multiple_of(core * head_width, head_width), head_width)
    peer_rows = pl.ds(pl.multiple_of(other * head_width, head_width), head_width)
    joined = lambda ref: jnp.concatenate([ref[i] for i in range(pairs)], axis=1)
    mixed = jnp.dot(joined(att_own), wo[own_rows, :], preferred_element_type=F32)
    for copy in att_copies:
        copy.wait_recv()
    mixed = mixed + jnp.dot(joined(att_peer), wo[peer_rows, :], preferred_element_type=F32)
    out_ref[...] = mixed.astype(BF16)

    for copy in att_copies:
        copy.wait_send()
    tok_copy.wait_send()

    def drain_list(d, _):
        list_copy(d, me - d).wait_send()
        return 0

    lax.fori_loop(1, me + 1, drain_list, 0)

    def drain_rows(d, _):
        each(row_copy(0, d, me + d, me), lambda c: c.wait_send())
        each(row_copy(1, d, me + d, me), lambda c: c.wait_send())
        return 0

    lax.fori_loop(1, devices - me, drain_rows, 0)

    @pl.when(me == 0)
    def _():
        def drain_root(d, _):
            root_copy(0, d).wait_send()
            root_copy(1, d).wait_send()
            return 0

        lax.fori_loop(1, direct + 1, drain_root, 0)

    if relayed:

        @pl.when(relay_here)
        def _():
            for kind in range(2):
                root_copy(kind, devices - 1, True).wait_send()


def quad_layer(
    chosen_hbm, tab_hbm, tok_hbm, wq_hbm, wk_hbm, wv_hbm, wo_hbm,
    out_ref,
    chosen_ref, tab, tok_own, tok_peer, wq, wk, wv, wo, q_acc, k_acc, v_acc, k_own, v_own, q2,
    lists, picks, k_rows, v_rows, far, peak, total, summed, weigh, mixed, att_own, att_peer,
    k_serve, v_serve, far_serve, q_out, q_in, state_out, state_in,
    load_sem, tok_send, tok_recv, att_send, att_recv, list_send, list_recv, key_send, key_recv, root_recv,
    wire_send, wire_recv,
):
    devices, server = 4, 1
    me = lax.axis_index("kv")
    core = lax.axis_index("tp")
    rows, half = tok_own.shape
    pairs = k_own.shape[0]
    picked = CAP * BLOCK
    other = 1 - core
    served = list(range(pairs - q_out.shape[0], pairs))
    plain = list(range(pairs - q_out.shape[0]))
    clients = [2, 3]
    buffers = ((k_own, k_rows), (v_own, v_rows))
    serves = (k_serve, v_serve)

    chosen_load, tok_load, tab_load, wk_load, wv_load, wq_load, wo_load = [
        pltpu.make_async_copy(src, dst, load_sem.at[i])
        for i, (src, dst) in enumerate(
            ((chosen_hbm, chosen_ref), (tok_hbm, tok_own), (tab_hbm, tab), (wk_hbm, wk), (wv_hbm, wv), (wq_hbm, wq), (wo_hbm, wo))
        )
    ]
    chosen_load.start()
    tok_load.start()

    @pl.when(me < 2)
    def _():
        for load in (wk_load, tab_load, wv_load, wq_load):
            load.start()

    @pl.when(me >= 2)
    def _():
        for load in (wq_load, tab_load, wk_load, wv_load):
            load.start()

    wo_load.start()

    barrier = pltpu.get_barrier_semaphore()
    pl.semaphore_signal(barrier, inc=1, device_id={"tp": other}, device_id_type=MESH)

    def greet(d, _):
        pl.semaphore_signal(barrier, inc=1, device_id={"kv": d}, device_id_type=MESH)
        return 0

    lax.fori_loop(me + 1, devices, greet, 0)

    for _, buffer in buffers:
        for slot in range(devices - 1):
            empty = slice(slot * LANES + picked, (slot + 1) * LANES)
            buffer[:, empty, :] = jnp.zeros((pairs, LANES - picked, LANES), BF16)
    for buffer in serves:
        shape = buffer.shape[:2] + (LANES - picked, LANES)
        buffer[:, :, slice(picked, LANES), :] = jnp.zeros(shape, BF16)

    own_half = pl.ds(pl.multiple_of(core * half, half), half)
    peer_half = pl.ds(pl.multiple_of(other * half, half), half)

    def list_copy(d):
        return pltpu.make_async_remote_copy(
            src_ref=chosen_ref, dst_ref=lists.at[d - 1], send_sem=list_send.at[0],
            recv_sem=list_recv.at[d - 1], device_id={"kv": jnp.maximum(me - d, 0)}, device_id_type=MESH,
        )

    tok_copy = pltpu.make_async_remote_copy(
        src_ref=tok_own, dst_ref=tok_peer, send_sem=tok_send.at[0],
        recv_sem=tok_recv.at[0], device_id={"tp": other}, device_id_type=MESH,
    )

    chosen_load.wait()
    pl.semaphore_wait(barrier, 1 + me)
    for d in range(1, devices):
        pl.when(me >= d)(lambda d=d: list_copy(d).start())
    tok_load.wait()
    tok_copy.start()

    lane = lax.broadcasted_iota(jnp.int32, (rows, LANES), 1)
    first = (lane % HEAD_DIM) < HEAD_DIM // 2
    row_i = lax.broadcasted_iota(jnp.int32, (rows, rows), 0)
    col_i = lax.broadcasted_iota(jnp.int32, (rows, rows), 1)
    earlier = jnp.where((row_i % BLOCK == 0) & (row_i // BLOCK < col_i // BLOCK), 1.0, 0.0).astype(BF16)

    def turn_tables():
        tab_load.wait()
        base = tab[pl.ds(rows + me, 1), :]
        row_cos, row_sin = tab[:rows, :LANES], tab[:rows, LANES:]
        base_cos, base_sin = base[:, :LANES], base[:, LANES:]
        cosine = row_cos * base_cos - row_sin * base_sin
        sine = row_sin * base_cos + row_cos * base_sin
        tab[:rows, :LANES] = cosine
        tab[:rows, LANES:] = jnp.where(first, -sine, sine)

    def rotated(x):
        swapped = jnp.where(
            first,
            pltpu.roll(x, LANES - HEAD_DIM // 2, axis=1),
            pltpu.roll(x, HEAD_DIM // 2, axis=1),
        )
        return x * tab[:rows, :LANES] + swapped * tab[:rows, LANES:]

    def begin(acc, weight):
        acc[...] = jnp.dot(tok_own[...], weight[own_half, :], preferred_element_type=F32)

    def rest(acc, weight, some):
        columns = slice(some[0] * LANES, (some[-1] + 1) * LANES)
        full = acc[:, columns] + jnp.dot(tok_peer[...], weight[peer_half, columns], preferred_element_type=F32)
        return [full[:, n * LANES : (n + 1) * LANES] for n in range(len(some))]

    def make_keys(some):
        for i, x in zip(some, rest(k_acc, wk, some)):
            k_own[i] = rotated(x).astype(BF16)

    def make_values(some):
        for i, x in zip(some, rest(v_acc, wv, some)):
            v_own[i] = x.astype(BF16)

    def make_queries(some, share=False):
        for i, x in zip(some, rest(q_acc, wq, some)):
            q = rotated(x).astype(BF16).astype(F32) * (HEAD_DIM**-0.5)
            if share:
                q_out[i - served[0]] = q.astype(BF16)
            q2[i, :rows, :] = jnp.where(lane < HEAD_DIM, q, 0.0).astype(BF16)
            q2[i, rows:, :] = jnp.where(lane < HEAD_DIM, 0.0, q).astype(BF16)

    def choose(m, t):
        list_copy(t - m).wait_recv()
        slot = slice((t - 1) * LANES, t * LANES)
        picks[slot, :] = selection(listed_columns(lists[t - m - 1], me, rows), earlier, LANES)

    def gather(sources, low, high):
        wide = jnp.concatenate([ref[i] for ref, i in sources], axis=1)
        got = jnp.dot(
            picks[(low - 1) * LANES : high * LANES, :], wide, preferred_element_type=F32
        ).astype(BF16)
        return [got[:, n * LANES : (n + 1) * LANES] for n in range(len(sources))]

    def row_copy(kind, i, m, t):
        buffer = buffers[kind][1]
        low = BLOCK if m == 0 else 0
        return pltpu.make_async_remote_copy(
            src_ref=buffer.at[i, slice((t - 1) * LANES + low, (t - 1) * LANES + picked)],
            dst_ref=buffer.at[i, slice((t - m - 1) * LANES + low, (t - m - 1) * LANES + picked)],
            send_sem=key_send.at[kind], recv_sem=key_recv.at[kind, i],
            device_id={"kv": t}, device_id_type=MESH,
        )

    def serve_copy(kind, i, c):
        return pltpu.make_async_remote_copy(
            src_ref=buffers[kind][1].at[i, slice((c - 1) * LANES + BLOCK, (c - 1) * LANES + picked)],
            dst_ref=serves[kind].at[i - served[0], c - 2, slice(BLOCK, picked)],
            send_sem=key_send.at[kind], recv_sem=wire_recv.at[len(served) + i - served[0], c - 2],
            device_id={"kv": server}, device_id_type=MESH,
        )

    def root_copy(kind, some, t, passing=False):
        own, buffer = buffers[kind]
        part = slice(some[0], some[-1] + 1)
        here = lambda slot: buffer.at[part, slice((slot - 1) * LANES, (slot - 1) * LANES + BLOCK)]
        return pltpu.make_async_remote_copy(
            src_ref=here(t - 1) if passing else own.at[part, slice(0, BLOCK)], dst_ref=here(t),
            send_sem=key_send.at[kind], recv_sem=root_recv.at[kind, 1 if some is served else 0],
            device_id={"kv": t}, device_id_type=MESH,
        )

    def query_copy(i):
        n = i - served[0]
        return pltpu.make_async_remote_copy(
            src_ref=q_out.at[n], dst_ref=q_in.at[n, jnp.maximum(me - 2, 0)],
            send_sem=wire_send.at[0], recv_sem=wire_recv.at[n, jnp.maximum(me - 2, 0)],
            device_id={"kv": server}, device_id_type=MESH,
        )

    def query_arrived(i, c):
        n = i - served[0]
        space = q_in.at[n, c - 2]
        pltpu.make_async_copy(space, space, wire_recv.at[n, c - 2]).wait()

    def state_copy(i, c):
        n = i - served[0]
        return pltpu.make_async_remote_copy(
            src_ref=state_out.at[n, c - 2], dst_ref=state_in.at[n],
            send_sem=wire_send.at[0], recv_sem=wire_recv.at[n, 0],
            device_id={"kv": c}, device_id_type=MESH,
        )

    everything = list(range(pairs))

    @pl.when(me == 0)
    def _():
        wk_load.wait()
        begin(k_acc, wk)
        turn_tables()
        wv_load.wait()
        begin(v_acc, wv)
        tok_copy.wait_recv()
        make_keys(everything)
        make_values(everything)
        choose(0, 1)
        for kind in range(2):
            root_copy(kind, served, 1).start()
        choose(0, 2)
        for kind in range(2):
            root_copy(kind, plain, 2).start()
        choose(0, 3)

        def pick(i):
            for (_, buffer), got in zip(buffers, gather([(k_own, i), (v_own, i)], 1, 3)):
                buffer[i] = got

        for step in range(max(len(served), len(plain))):
            for i in served[step : step + 1]:
                pick(i)
                for c in clients:
                    for kind in range(2):
                        serve_copy(kind, i, c).start()
                for kind in range(2):
                    row_copy(kind, i, 0, 1).start()
            for i in plain[step : step + 1]:
                pick(i)
                for kind in range(2):
                    for t in (2, 3):
                        row_copy(kind, i, 0, t).start()
        for kind in range(2):
            root_copy(kind, plain, 1).start()
            for i in plain:
                row_copy(kind, i, 0, 1).start()
        wq_load.wait()
        begin(q_acc, wq)
        make_queries(everything)

    @pl.when(me == 1)
    def _():
        wk_load.wait()
        begin(k_acc, wk)
        turn_tables()
        wv_load.wait()
        begin(v_acc, wv)
        tok_copy.wait_recv()

        def pass_on(kind, t):
            own, buffer = buffers[kind]
            slot = slice((t - 1) * LANES, t * LANES)
            for i, got in zip(plain, gather([(own, i) for i in plain], t, t)):
                buffer[i, slot, :] = got
            for i in plain:
                row_copy(kind, i, 1, t).start()

        make_keys(plain)
        choose(1, 2)
        pass_on(0, 2)
        make_values(plain)
        pass_on(1, 2)
        choose(1, 3)
        pass_on(0, 3)
        pass_on(1, 3)
        make_keys(served)
        make_values(served)
        for i in served:
            for buffer, got in zip(serves, gather([(k_own, i), (v_own, i)], 2, 3)):
                for c in clients:
                    buffer[i - served[0], c - 2, LANES : 2 * LANES, :] = got[(c - 2) * LANES : (c - 1) * LANES]
        wq_load.wait()
        begin(q_acc, wq)
        make_queries(everything)

    @pl.when(me >= 2)
    def _():
        wq_load.wait()
        begin(q_acc, wq)
        turn_tables()
        wk_load.wait()
        begin(k_acc, wk)
        tok_copy.wait_recv()
        make_queries(served, True)
        query_copy(served[0]).start()
        make_keys(everything)
        for i in served[1:]:
            query_copy(i).start()

        def pass_on(kind):
            @pl.when(me == 2)
            def _():
                own, buffer = buffers[kind]
                if kind == 0:
                    choose(2, 3)
                for i, got in zip(everything, gather([(own, i) for i in everything], 3, 3)):
                    buffer[i, 2 * LANES :, :] = got
                for i in served + plain:
                    row_copy(kind, i, 2, 3).start()

        pass_on(0)
        wv_load.wait()
        begin(v_acc, wv)
        make_values(everything)
        pass_on(1)
        make_queries(plain)

    chosen = chosen_ref[...]

    def spread(hit):
        keys = hit.shape[1]
        blocks = hit.shape[0]
        wide = jnp.broadcast_to(hit[:, None, :], (blocks, BLOCK, keys))
        return wide.reshape(blocks * BLOCK, keys)

    def scores_of(queries, keys):
        return lax.dot_general(queries, keys, (((1,), (1,)), ((), ())), preferred_element_type=F32)

    def lane_sums(weights):
        return sum(weights[:, j : j + LANES] for j in range(0, weights.shape[1], LANES))

    def twice(x):
        return jnp.concatenate([x, x], axis=0)

    listed = spread(listed_columns(chosen, me, rows))
    bias = twice(jnp.where((listed > 0.5) & (col_i <= row_i), 0.0, MASKED))
    for i in everything:
        scores = scores_of(q2[i], k_own[i]) + bias
        top = jnp.max(scores, axis=1, keepdims=True)
        weights = jnp.exp(scores - top)
        peak[i] = jnp.broadcast_to(top, peak.shape[1:])
        total[i] = lane_sums(weights)
        summed[i] = jnp.dot(weights.astype(BF16), v_own[i], preferred_element_type=F32)

    def mask_of(wanted, holder):
        hit = listed_columns(wanted, holder, rows)
        pick = selection(hit, earlier, LANES)
        got = lax.dot_general(
            hit.astype(BF16), pick, (((1,), (1,)), ((), ())), preferred_element_type=F32
        )
        return jnp.where(spread(got) > 0.5, 0.0, MASKED)

    @pl.when(me == server)
    def _():
        for c in clients:
            for holder in range(2):
                far_serve[c - 2, :, holder * LANES : (holder + 1) * LANES] = mask_of(lists[c - 2], holder)

    @pl.when(me == 2)
    def _():
        for kind in range(2):
            root_copy(kind, plain, 2).wait_recv()
            root_copy(kind, plain, 3, True).start()

    for d in range(1, devices):

        @pl.when(me >= d)
        def _(d=d):
            far[:, (d - 1) * LANES : d * LANES] = mask_of(chosen, me - d)

    def att_copy(i):
        return pltpu.make_async_remote_copy(
            src_ref=att_own.at[i], dst_ref=att_peer.at[i], send_sem=att_send.at[0],
            recv_sem=att_recv.at[i], device_id={"tp": other}, device_id_type=MESH,
        )

    def finish(i, merged):
        att_own[i] = merged.astype(BF16)
        att_copy(i).start()

    def by_head(result):
        return jnp.where(lane < HEAD_DIM, result[:rows], result[rows:])

    def product(i):
        att_copy(i).wait_recv()
        both = jnp.concatenate([att_own[i], att_peer[i]], axis=1)
        weight = jnp.concatenate(
            [
                wo[pl.ds(pl.multiple_of((device * pairs + i) * LANES, LANES), LANES), :]
                for device in (core, other)
            ],
            axis=0,
        )
        return jnp.dot(both, weight, preferred_element_type=F32)

    def project(order, low, high):
        for n in range(low, high):
            got = product(order[n])
            if n > 0:
                got = mixed[...] + got
            if n == pairs - 1:
                out_ref[...] = got.astype(BF16)
            else:
                mixed[...] = got

    def arrived(kind, i, count):
        space = buffers[kind][1].at[i, slice(0, count)]
        pltpu.make_async_copy(space, space, key_recv.at[kind, i]).wait()

    def key_part(m, i, n):
        arrived(0, i, m * picked - BLOCK)
        keys = slice(0, m * LANES)
        scores = scores_of(q2[i], k_rows[i, keys, :]) + twice(far[:, keys])
        old = peak[i]
        top = jnp.maximum(old, jnp.max(scores, axis=1, keepdims=True))
        factor = jnp.exp(old - top)
        weights = jnp.exp(scores - jnp.concatenate([top] * m, axis=1))
        inverse = 1.0 / jnp.sum(total[i] * factor + lane_sums(weights), axis=1, keepdims=True)
        summed[i] = summed[i] * (factor * inverse)
        total[i] = jnp.broadcast_to(inverse, total.shape[1:])
        weigh[n, :, keys] = weights.astype(BF16)

    def value_part(m, i, n):
        arrived(1, i, m * picked - BLOCK)
        keys = slice(0, m * LANES)
        after = jnp.dot(weigh[n, :, keys], v_rows[i, keys, :], preferred_element_type=F32)
        finish(i, by_head(summed[i] + after * total[i]))

    eye = lax.broadcasted_iota(jnp.int32, (LANES, LANES), 0) == lax.broadcasted_iota(jnp.int32, (LANES, LANES), 1)
    strips = 2 * rows // LANES

    def serve(i, c):
        n = i - served[0]
        query_arrived(i, c)
        space = k_rows.at[i, slice(0, 2 * (picked - BLOCK))]
        pltpu.make_async_copy(space, space, wire_recv.at[len(served) + n, c - 2]).wait()
        for kind in range(2):
            serves[kind][n, c - 2, :BLOCK, :] = buffers[kind][1][i, :BLOCK, :]
        q = q_in[n, c - 2].astype(F32)
        q = jnp.concatenate(
            [jnp.where(lane < HEAD_DIM, q, 0.0), jnp.where(lane < HEAD_DIM, 0.0, q)], axis=0
        ).astype(BF16)
        scores = scores_of(q, k_serve[n, c - 2]) + twice(far_serve[c - 2])
        top = jnp.max(scores, axis=1, keepdims=True)
        weights = jnp.exp(scores - top)
        mass = jnp.sum(lane_sums(weights), axis=1, keepdims=True)
        result = jnp.dot(weights.astype(BF16), v_serve[n, c - 2], preferred_element_type=F32)
        state_out[n, c - 2, :rows, :] = by_head(result * (1.0 / mass)).astype(BF16)
        level = top + jnp.log(mass)
        strip = jnp.concatenate(
            [
                jnp.sum(jnp.where(eye, level[j * LANES : (j + 1) * LANES], 0.0), axis=0, keepdims=True)
                for j in range(strips)
            ],
            axis=0,
        )
        high = strip.astype(BF16).astype(F32)
        middle = (strip - high).astype(BF16).astype(F32)
        low = strip - high - middle
        spare = jnp.zeros((state_out.shape[2] - rows - 3 * strips, LANES), F32)
        state_out[n, c - 2, rows:, :] = jnp.concatenate([high, middle, low, spare], axis=0).astype(BF16)
        state_copy(i, c).start()

    def fold(i):
        for kind in range(2):
            arrived(kind, i, picked)
        scores = scores_of(q2[i], k_rows[i, :LANES, :]) + twice(far[:, :LANES])
        old = peak[i]
        top = jnp.maximum(old, jnp.max(scores, axis=1, keepdims=True))
        factor = jnp.exp(old - top)
        weights = jnp.exp(scores - top)
        peak[i] = top
        total[i] = total[i] * factor + weights
        summed[i] = summed[i] * factor + jnp.dot(
            weights.astype(BF16), v_rows[i, :LANES, :], preferred_element_type=F32
        )

    def merge(i):
        n = i - served[0]
        mass = jnp.sum(total[i], axis=1, keepdims=True)
        state_copy(i, 2).wait_recv()
        tail = state_in[n, rows:, :].astype(F32)
        strip = tail[:strips] + tail[strips : 2 * strips] + tail[2 * strips : 3 * strips]
        level = jnp.concatenate(
            [
                jnp.sum(jnp.where(eye, strip[j : j + 1], 0.0), axis=1, keepdims=True)
                for j in range(strips)
            ],
            axis=0,
        )
        old = peak[i]
        top = jnp.maximum(old, level)
        factor, share = jnp.exp(old - top), jnp.exp(level - top)
        inverse = 1.0 / (mass * factor + share)
        there = state_in[n, :rows, :].astype(F32)
        finish(i, by_head(summed[i] * (factor * inverse)) + there * by_head(share * inverse))

    wo_load.wait()

    @pl.when(me == 0)
    def _():
        for i in everything:
            finish(i, by_head(summed[i] / jnp.sum(total[i], axis=1, keepdims=True)))
        project(everything, 0, pairs)

    @pl.when(me == server)
    def _():
        for kind in range(2):
            root_copy(kind, served, 1).wait_recv()
        for i in served:
            for c in clients:
                serve(i, c)
            key_part(1, i, 0)
            value_part(1, i, 0)
        order = served + plain
        for kind in range(2):
            root_copy(kind, plain, 1).wait_recv()
        for n, i in enumerate(plain):
            key_part(1, i, n)
        project(order, 0, len(served))
        for n, i in enumerate(plain):
            value_part(1, i, n)
        project(order, len(served), pairs)

    for m in clients:

        @pl.when(me == m)
        def _(m=m):
            if m == 3:
                for i in served:
                    fold(i)
                root_copy(0, plain, 3).wait_recv()
            for n, i in enumerate(plain):
                key_part(m, i, n)
            if m == 3:
                root_copy(1, plain, 3).wait_recv()
            for n, i in enumerate(plain):
                value_part(m, i, n)
            merge(served[0])
            project(everything, 0, len(plain))
            for i in served[1:]:
                merge(i)
            project(everything, len(plain), pairs)

    def settle(space, semaphore):
        pltpu.make_async_copy(space, space, semaphore).wait()

    settle(att_own, att_send.at[0])
    settle(tok_own, tok_send.at[0])
    for m in range(1, devices):

        @pl.when(me == m)
        def _(m=m):
            settle(lists.at[slice(0, m)], list_send.at[0])

    @pl.when(me == server)
    def _():
        settle(state_out, wire_send.at[0])

    @pl.when(me >= 2)
    def _():
        settle(q_out, wire_send.at[0])

    fresh = picked - BLOCK
    sent = {
        0: [pairs * BLOCK + len(plain) * BLOCK + pairs * 3 * fresh],
        1: [len(plain) * 2 * picked],
        2: [len(plain) * BLOCK + pairs * picked],
    }
    width = (devices - 1) * LANES
    for m, (count,) in sent.items():

        @pl.when(me == m)
        def _(count=count):
            for kind in range(2):
                buffer = buffers[kind][1]
                whole = count // pairs
                settle(buffer.at[:, slice(0, whole)], key_send.at[kind])


def quad_call(tokens, query_weight, key_weight, value_weight, out_weight, chosen):
    devices = 4
    rows, half = tokens.shape
    width, head_width = query_weight.shape
    pairs = head_width // LANES
    table = np.concatenate(rotary_tables(rows, devices), axis=0)
    vmem = pl.BlockSpec(memory_space=pltpu.VMEM)
    anywhere = pl.BlockSpec(memory_space=pl.ANY)
    dma = pltpu.SemaphoreType.DMA
    served = pairs // 2
    others = devices - 1
    strips = 2 * rows // LANES
    state = rows + -(-3 * strips // 16) * 16
    return pl.pallas_call(
        quad_layer,
        out_shape=pltpu.VMEM((rows, out_weight.shape[1]), BF16),
        in_specs=[anywhere] * 7,
        out_specs=vmem,
        scratch_shapes=[
            pltpu.VMEM(chosen.shape, jnp.int32),
            pltpu.VMEM(table.shape, F32),
            pltpu.VMEM((rows, half), BF16),
            pltpu.VMEM((rows, half), BF16),
            pltpu.VMEM((width, head_width), BF16),
            pltpu.VMEM((width, head_width), BF16),
            pltpu.VMEM((width, head_width), BF16),
            pltpu.VMEM(out_weight.shape, BF16),
            pltpu.VMEM((rows, head_width), F32),
            pltpu.VMEM((rows, head_width), F32),
            pltpu.VMEM((rows, head_width), F32),
            pltpu.VMEM((pairs, rows, LANES), BF16),
            pltpu.VMEM((pairs, rows, LANES), BF16),
            pltpu.VMEM((pairs, 2 * rows, LANES), BF16),
            pltpu.VMEM((others,) + chosen.shape, jnp.int32),
            pltpu.VMEM((others * LANES, rows), BF16),
            pltpu.VMEM((pairs, others * LANES, LANES), BF16),
            pltpu.VMEM((pairs, others * LANES, LANES), BF16),
            pltpu.VMEM((rows, others * LANES), F32),
            pltpu.VMEM((pairs, 2 * rows, LANES), F32),
            pltpu.VMEM((pairs, 2 * rows, LANES), F32),
            pltpu.VMEM((pairs, 2 * rows, LANES), F32),
            pltpu.VMEM((pairs, 2 * rows, others * LANES), BF16),
            pltpu.VMEM((rows, out_weight.shape[1]), F32),
            pltpu.VMEM((pairs, rows, LANES), BF16),
            pltpu.VMEM((pairs, rows, LANES), BF16),
            pltpu.VMEM((served, 2, 2 * LANES, LANES), BF16),
            pltpu.VMEM((served, 2, 2 * LANES, LANES), BF16),
            pltpu.VMEM((2, rows, 2 * LANES), F32),
            pltpu.VMEM((served, rows, LANES), BF16),
            pltpu.VMEM((served, 2, rows, LANES), BF16),
            pltpu.VMEM((served, 2, state, LANES), BF16),
            pltpu.VMEM((served, state, LANES), BF16),
            dma((7,)),
            dma((1,)),
            dma((1,)),
            dma((1,)),
            dma((pairs,)),
            dma((1,)),
            dma((others,)),
            dma((2,)),
            dma((2, pairs)),
            dma((2, 2)),
            dma((1,)),
            dma((2 * served, 2)),
        ],
        compiler_params=pltpu.CompilerParams(
            collective_id=0, has_side_effects=True, vmem_limit_bytes=62 * 1024 * 1024
        ),
        name="layer",
    )(chosen, jnp.asarray(table), tokens, query_weight, key_weight, value_weight, out_weight)


def on_device(devices, tokens, query_weight, key_weight, value_weight, out_weight, chosen):
    rows, half = tokens.shape
    width, head_width = query_weight.shape
    pairs = head_width // LANES
    picked = CAP * BLOCK
    if devices == 4 and pairs % 2 == 0:
        return quad_call(tokens, query_weight, key_weight, value_weight, out_weight, chosen)
    row_table, base_table = rotary_tables(rows, devices)
    vmem = pl.BlockSpec(memory_space=pltpu.VMEM)
    anywhere = pl.BlockSpec(memory_space=pl.ANY)
    dma = pltpu.SemaphoreType.DMA
    return pl.pallas_call(
        functools.partial(layer, devices),
        out_shape=pltpu.VMEM((rows, out_weight.shape[1]), BF16),
        in_specs=[anywhere] * 8,
        out_specs=vmem,
        scratch_shapes=[
            pltpu.VMEM(chosen.shape, jnp.int32),
            pltpu.VMEM(base_table.shape, F32),
            pltpu.VMEM((rows, 2 * LANES), F32),
            pltpu.VMEM((rows, half), BF16),
            pltpu.VMEM((rows, half), BF16),
            pltpu.VMEM((width, head_width), BF16),
            pltpu.VMEM((width, head_width), BF16),
            pltpu.VMEM((width, head_width), BF16),
            pltpu.VMEM(out_weight.shape, BF16),
            pltpu.VMEM((rows, head_width), F32),
            pltpu.VMEM((rows, head_width), F32),
            pltpu.VMEM((rows, head_width), F32),
            pltpu.VMEM((rows, head_width), BF16),
            pltpu.VMEM((rows, head_width), BF16),
            pltpu.VMEM((pairs, 2 * rows, LANES), BF16),
            pltpu.VMEM((devices,) + chosen.shape, jnp.int32),
            pltpu.VMEM((devices, picked, rows), BF16),
            pltpu.VMEM((devices, picked, head_width), BF16),
            pltpu.VMEM((devices, picked, head_width), BF16),
            pltpu.VMEM((devices - 1, pairs, 2 * rows, picked), F32),
            pltpu.VMEM((pairs, 2 * rows, picked), F32),
            pltpu.VMEM((pairs, 2 * rows, LANES), F32),
            pltpu.VMEM((pairs, 2 * rows, LANES), F32),
            pltpu.VMEM((pairs, 2 * rows, LANES), F32),
            pltpu.VMEM((pairs, 2 * rows, picked), BF16),
            pltpu.VMEM((pairs, rows, LANES), BF16),
            pltpu.VMEM((pairs, rows, LANES), BF16),
            dma((8,)),
            dma((2,)),
            dma((2, pairs)),
            dma((devices,)),
            dma((devices,)),
            dma((2, devices)),
            dma((2, devices)),
            dma((2, devices)),
            dma((2,)),
        ],
        compiler_params=pltpu.CompilerParams(
            collective_id=0, has_side_effects=True, vmem_limit_bytes=62 * 1024 * 1024
        ),
        name="layer",
    )(
        chosen, jnp.asarray(base_table), jnp.asarray(row_table), tokens,
        query_weight, key_weight, value_weight, out_weight,
    )


def solution(mesh):
    placed = (
        P(("dp", "kv"), "tp"),
        P(None, "tp"),
        P(None, "tp"),
        P(None, "tp"),
        P(None, "tp"),
        P(("dp", "kv"), None),
    )
    return jax.shard_map(
        functools.partial(on_device, mesh.shape["kv"]),
        mesh=mesh, in_specs=placed, out_specs=P(("dp", "kv"), "tp"), check_vma=False,
    )
```
